256 devices in a mesh: gr: 2 (over z_hi), sp: 16 (over z_lo, x), tp: 8 (over y, core).
Axes of the slice: x: 4, y: 4, z: 8 (z_hi: 2, z_lo: 4; z = z_hi * 4 + z_lo), core: 2. Of those that a mesh axis runs over, the one named last changes fastest.
Arguments:
- tokens: bfloat16 [8, 65536, 2048], P('gr', ('sp', 'tp')), parts along dimension 0, may hold values from -6 to 6
- norm_gain: float32 [2048], replicated, may hold values from 0.1 to 1.9
- w_key: bfloat16 [2048, 256], replicated, may hold values from -0.125 to 0.125
- w_value: bfloat16 [2048, 256], replicated, may hold values from -0.125 to 0.125
- new_query: bfloat16 [8, 32, 64], P('gr'), parts along dimension 0, may hold values from -360 to 360
- cum_gate: float32 [32, 8, 8192], P(('gr', 'sp'), 'tp'), parts along dimension 0, may hold values from -8193 to 0, as said below
Outputs:
- kv_cache: bfloat16 [32, 8, 8192, 128], P(('gr', 'sp'), 'tp'), parts along dimension 0
- first_read: float32 [8, 32, 64], P('gr'), parts along dimension 0
The draws below stay inside these ranges and needn't reach their ends.
There are 2 independent parts, one for each index of `gr`. The reference program is written for one: setup_inputs(seed, part) draws one part's arguments, and reference() takes and returns one part's arrays. A program takes and returns all parts, laid end to end along the dimension named above; an argument that names none is the same for every part. Nothing has to cross between parts.
Inputs may be any that keep to these rules, and one draw needn't show every extreme that they name: `cum_gate`: for each sequence and key head, the running sum along the positions of the sequence of negative log forget gates; it never rises from one position to the next.
All inputs are finite; a program needn't handle non-finite values.
Results may differ from the reference program's by a relative error of at most 0.0014.
The reference program's roundings to bfloat16 on the way (of `normed`, `keys_all` and `values_all`) count: a program that leaves them out, or rounds other values in their place, can miss the bound.
Values may be sent and summed in bfloat16 or wider, within the bound.
A program may use at most 64 MiB of HBM per device.

```python
from functools import partial
import jax
import jax.numpy as jnp
from jax import lax

D = 2048
HD = 64
QH = 32
KVH = 4
SEQS = 4
POS_DEV = 512
BLOCKS = 128
LEN = 65536
CLASSES = 4
HALVES = 2
PIECE = 64


def draw_new_query(key, part):
    base = 3.0 * jax.random.normal(jax.random.fold_in(key, 3), (SEQS, QH, HD), jnp.float32)
    base = jnp.clip(base, -18.0, 18.0)
    return base.astype(jnp.bfloat16)


def draw_cum_gate(key, part):
    flag_key = jax.random.fold_in(key, 11)
    fast_flags = jax.random.randint(flag_key, (SEQS, KVH, 1, 1), 0, 2) == 1
    fast_rate = jnp.exp(jax.random.uniform(jax.random.fold_in(key, 12), (SEQS, KVH, 1, 1), jnp.float32, jnp.log(0.01), jnp.log(1.0 / 30.0)))
    slow_rate = jnp.exp(jax.random.uniform(jax.random.fold_in(key, 13), (SEQS, KVH, 1, 1), jnp.float32, jnp.log(0.3), jnp.log(1.0))) / LEN
    base_rate = jnp.where(fast_flags, fast_rate, slow_rate)
    block_factor = jnp.exp(jax.random.uniform(jax.random.fold_in(key, 14), (SEQS, KVH, BLOCKS, 1), jnp.float32, jnp.log(0.5), jnp.log(2.0)))
    jitter = jax.random.uniform(jax.random.fold_in(key, 15), (SEQS, KVH, BLOCKS, POS_DEV), jnp.float32, 0.25, 1.75)
    log_gate = -(base_rate * block_factor * jitter)
    running = jnp.cumsum(log_gate.reshape(SEQS, KVH, LEN), axis=-1)
    laid = running.reshape(SEQS, KVH, BLOCKS, CLASSES, HALVES, PIECE).transpose(0, 3, 1, 4, 2, 5)
    return laid.reshape(SEQS * CLASSES, KVH * HALVES, BLOCKS * PIECE)


def block_levels(key, dims, cuts, least, high):
    loudness = 1.0
    for dim, parts in cuts:
        heights = jax.random.uniform(jax.random.fold_in(jax.random.fold_in(key, 6), dim), (parts,), jnp.float32, least / len(cuts), high / len(cuts))
        loudness = loudness * jnp.repeat(jnp.exp(heights), dims[dim] // parts).reshape((-1,) + (1,) * (len(dims) - 1 - dim))
    return loudness


def bell_draw(rng, shape, deviation, reach, split=(), kind=jnp.bfloat16):
    factor_of = block_levels(rng, shape, split, -0.22, 0.18) if split else 1.0
    values = jax.random.normal(rng, shape, jnp.float32) * deviation * factor_of
    return jnp.minimum(jnp.maximum(values, -reach), reach).astype(kind)


def setup_inputs(seed: int = 0, part: int = 0) -> dict:
    key_of = jax.random.split(jax.random.key(seed), 7)
    part_splits = jax.random.split(jax.random.fold_in(key_of[6], part), 7)
    return {
        "tokens": bell_draw(part_splits[0], (SEQS, LEN, D), 1.0, 6.0, ((1, 128),)),
        "norm_gain": jnp.clip(1.0 + 0.18 * jax.random.normal(key_of[1], (D,), jnp.float32), 0.1, 1.9),
        "w_key": bell_draw(key_of[2], (D, KVH * HD), D ** -0.5, 0.125),
        "w_value": bell_draw(key_of[3], (D, KVH * HD), D ** -0.5, 0.125),
        "new_query": draw_new_query(jax.random.fold_in(jax.random.fold_in(key_of[6], part), 71), part),
        "cum_gate": draw_cum_gate(jax.random.fold_in(jax.random.fold_in(key_of[6], part), 71), part),
    }


NORM_FLOOR = 0.05

def project_block(norm_gain, w_key, w_value, pos_block):
    widened = pos_block.astype(jnp.float32)
    inverse_rms = lax.rsqrt(lax.optimization_barrier(jnp.mean(widened * widened, axis=-1, keepdims=True)) + NORM_FLOOR)
    normed = (widened * inverse_rms * norm_gain.astype(jnp.float32)).astype(jnp.bfloat16)
    keys_made = jnp.dot(normed, w_key, preferred_element_type=jnp.float32).astype(jnp.bfloat16)
    values_made = jnp.dot(normed, w_value, preferred_element_type=jnp.float32).astype(jnp.bfloat16)
    keys_made = keys_made.reshape(POS_DEV, KVH, HD)
    values_made = values_made.reshape(POS_DEV, KVH, HD)
    return jnp.concatenate([keys_made, values_made], axis=-1)

def reference(tokens, norm_gain, w_key, w_value, new_query, cum_gate):
    pos_blocks = tokens.reshape(SEQS * BLOCKS, POS_DEV, D)
    stacked = lax.map(partial(project_block, norm_gain, w_key, w_value), pos_blocks)
    stacked = stacked.reshape(SEQS, BLOCKS, CLASSES, HALVES, PIECE, KVH, 2 * HD)
    kv_cache = stacked.transpose(0, 2, 5, 3, 1, 4, 6).reshape(SEQS * CLASSES, KVH * HALVES, BLOCKS * PIECE, 2 * HD)
    per_head = kv_cache.reshape(SEQS, CLASSES, KVH, HALVES, BLOCKS * PIECE, 2 * HD)
    per_head = per_head.transpose(0, 2, 1, 3, 4, 5).reshape(SEQS, KVH, LEN, 2 * HD)
    gates = cum_gate.reshape(SEQS, CLASSES, KVH, HALVES, BLOCKS * PIECE)
    gates = gates.transpose(0, 2, 1, 3, 4).reshape(SEQS, KVH, LEN)
    keys_all = per_head[..., :HD].astype(jnp.float32)
    values_all = per_head[..., HD:].astype(jnp.float32)
    grouped = new_query.astype(jnp.float32).reshape(SEQS, KVH, QH // KVH, HD)
    scores = jnp.einsum('sgqd,sgpd->sgqp', grouped, keys_all, precision=lax.Precision.HIGHEST)
    scores = scores * HD ** (-0.5) - gates[:, :, None, :]
    row_top = lax.optimization_barrier(jnp.max(scores, axis=-1, keepdims=True))
    weights = jnp.exp(scores - row_top)
    row_total = lax.optimization_barrier(jnp.sum(weights, axis=-1))
    summed = jnp.einsum('sgqp,sgpd->sgqd', weights, values_all, precision=lax.Precision.HIGHEST)
    first_read = (summed / row_total[..., None]).reshape(SEQS, QH, HD)
    return (kv_cache, first_read)
```

```python
import jax
import jax.numpy as jnp
from jax import lax
from jax.experimental import pallas as pl
from jax.experimental.pallas import tpu as pltpu
from jax.sharding import Mesh
from jax.sharding import PartitionSpec as P

HD = 64
AXES = ("sp_0", "sp_1", "tp_0", "tp_1")
SP_TP = AXES
SP = AXES[:2]
TP = AXES[2:]
GR_SP = ("gr", "sp_0", "sp_1")
MESH = pl.DeviceIdType.MESH
NORM_FLOOR = 0.05
SCORE_FLOOR = -1e30
ROWS = 128
STEPS = 16


def across(z, kz):
    flip = z + 1 - 2 * (z % 2)
    return ((1 - kz % 2) * z + (kz % 2) * flip + 2 * (kz // 2)) % 4


def peer_of(me, kz, kx, ky, kc):
    z, x, y, c = me
    return across(z, kz), (x + kx) % 4, (y + ky) % 4, (c + kc) % 2


def device_of(t):
    return dict(zip(AXES, t))


def slot_of(t):
    return t[0] * 32 + t[1] * 8 + t[2] * 2 + t[3]


def cache_kernel(
    tok_hbm, gain_ref, wk_hbm, wv_hbm, kv_hbm,
    tok, wk, wv, normed, made, tok_sem, w_sem, self_sem, send_sem, recv_sem,
):
    me = tuple(lax.axis_index(a) for a in AXES)
    mine = slot_of(me)
    wk_copy = pltpu.make_async_copy(wk_hbm, wk, w_sem.at[0])
    wv_copy = pltpu.make_async_copy(wv_hbm, wv, w_sem.at[1])

    def rel(i):
        return 3 - i % 4, (i // 4 + 1) % 4

    def tok_copy(i):
        kz, kx = rel(i)
        rows = pl.ds(pl.multiple_of((me[1] + kx) % 4 * ROWS, ROWS), ROWS)
        return pltpu.make_async_copy(
            tok_hbm.at[across(me[0], kz), rows], tok.at[i], tok_sem.at[i]
        )

    tok_copy(0).start()
    wk_copy.start()
    wv_copy.start()

    @pl.loop(1, STEPS)
    def _(i):
        tok_copy(i).start()

    barrier = pltpu.get_barrier_semaphore()

    @pl.loop(1, 128)
    def _(n):
        k = 128 - n
        to = peer_of(me, k // 32, k // 8 % 4, k // 2 % 4, k % 2)
        pl.semaphore_signal(barrier, inc=1, device_id=device_of(to), device_id_type=MESH)

    wk_copy.wait()
    wv_copy.wait()

    @pl.loop(0, STEPS)
    def _(i):
        kz, kx = rel(i)
        tok_copy(i).wait()

        for r in range(0, ROWS, 16):
            wide = tok[i, pl.ds(r, 16)].astype(jnp.float32)
            mean = jnp.sum(wide * wide, axis=-1, keepdims=True) * (1.0 / wide.shape[-1])
            scale = lax.rsqrt(mean + NORM_FLOOR)
            normed[pl.ds(r, 16)] = (wide * scale * gain_ref[...]).astype(jnp.bfloat16)

        keys = jnp.dot(normed[...], wk[...], preferred_element_type=jnp.float32)
        values = jnp.dot(normed[...], wv[...], preferred_element_type=jnp.float32)
        base = across(me[0], kz) * 32 + (me[1] + kx) % 4 * 8
        for h in range(4):
            cols = slice(h * HD, (h + 1) * HD)
            both = jnp.concatenate([keys[:, cols], values[:, cols]], axis=1).astype(jnp.bfloat16)
            made[base + 2 * h] = both[:64]
            made[base + 2 * h + 1] = both[64:]

        @pl.when(i == 0)
        def _():
            pl.semaphore_wait(barrier, 127)

        @pl.loop(0, 8)
        def _(j):
            to = peer_of(me, kz, kx, j // 2, j % 2)

            @pl.when(i * 8 + j != 120)
            def _():
                pltpu.make_async_remote_copy(
                    made.at[slot_of(to)], kv_hbm.at[mine], send_sem, recv_sem,
                    device_id=device_of(to), device_id_type=MESH,
                ).start()

    own = pltpu.make_async_copy(made.at[mine], kv_hbm.at[mine], self_sem)
    own.start()
    own.wait()
    some = pl.ds(0, 127)
    pltpu.make_async_copy(made.at[some], kv_hbm.at[some], recv_sem).wait()
    pltpu.make_async_copy(made.at[some], kv_hbm.at[some], send_sem).wait()


def make_cache(tokens, norm_gain, w_key, w_value):
    width = tokens.shape[-1]
    any_space = pl.BlockSpec(memory_space=pl.ANY)
    return pl.pallas_call(
        cache_kernel,
        out_shape=jax.ShapeDtypeStruct((128, 64, 2 * HD), jnp.bfloat16),
        in_specs=[any_space, pl.BlockSpec(memory_space=pltpu.VMEM), any_space, any_space],
        out_specs=any_space,
        scratch_shapes=[
            pltpu.VMEM((STEPS, ROWS, width), jnp.bfloat16),
            pltpu.VMEM(w_key.shape, jnp.bfloat16),
            pltpu.VMEM(w_value.shape, jnp.bfloat16),
            pltpu.VMEM((ROWS, width), jnp.bfloat16),
            pltpu.VMEM((128, 64, 2 * HD), jnp.bfloat16),
            pltpu.SemaphoreType.DMA((STEPS,)),
            pltpu.SemaphoreType.DMA((2,)),
            pltpu.SemaphoreType.DMA,
            pltpu.SemaphoreType.DMA,
            pltpu.SemaphoreType.DMA,
        ],
        compiler_params=pltpu.CompilerParams(collective_id=0, has_side_effects=True),
        cost_estimate=pl.CostEstimate(flops=4_300_000_000, bytes_accessed=14_000_000, transcendentals=0),
    )(tokens, norm_gain.reshape(1, -1), w_key, w_value)


def collected_together(array, axis):
    leaves = jax.tree.leaves(array)
    order = sorted(range(len(leaves)), key=lambda k: -leaves[k].size)
    width = (1, *leaves[order[0]].shape)[-1]
    lines = [
        jnp.pad(leaves[k].reshape(-1), (0, -leaves[k].size % width)).reshape(-1, width)
        for k in order
    ]
    both, at, found = (lax.all_gather(jnp.concatenate(lines), axis), 0, {})
    for k, line in zip(order, lines):
        slab = both[:, at : at + len(line)].reshape(len(both), -1)
        found[k] = slab[:, : leaves[k].size].reshape(-1, *leaves[k].shape)
        at += len(line)
    numbers = iter(range(len(leaves)))
    return jax.tree.map(lambda _: found[next(numbers)], array)


def merged_by_axis(array, axes, combine):
    for axis in axes:
        pieces = collected_together(array, axis)
        array = jax.tree.map(lambda part: part[0], pieces)
        for k in range(1, lax.axis_size(axis)):
            array = combine(array, jax.tree.map(lambda part: part[k], pieces))
    return array


def combine(left_side, right_side):
    out_left, top_left, sum_left = left_side
    out_right, top_right, sum_right = right_side
    merged_top = jnp.maximum(top_left, top_right)
    factor_left = jnp.exp(top_left - merged_top)
    factor_right = jnp.exp(top_right - merged_top)
    merged_out = out_left * factor_left[..., None] + out_right * factor_right[..., None]
    merged_sum = sum_left * factor_left + sum_right * factor_right
    return (merged_out, merged_top, merged_sum)


def shards(tokens, norm_gain, w_key, w_value, new_query, cum_gate):
    seq_count, positions, model_width = tokens.shape
    sp_count = lax.axis_size(SP)
    tp_count = lax.axis_size(TP)
    kv_heads = w_key.shape[1] // HD
    classes = sp_count // seq_count
    halves = tp_count // kv_heads
    piece_len = positions // (classes * halves)
    arrived = make_cache(tokens, norm_gain, w_key, w_value)
    kv_cache = arrived.reshape(1, 1, sp_count * tp_count * piece_len, 2 * HD)
    query_heads = new_query.shape[1]
    group_size = query_heads // kv_heads
    seq_index = lax.axis_index(SP) // classes
    head_index = lax.axis_index(TP) // halves
    queries = lax.dynamic_slice(
        new_query, (seq_index, head_index * group_size, 0), (1, group_size, HD)
    )[0]
    keys_here = kv_cache[0, 0, :, :HD]
    values_here = kv_cache[0, 0, :, HD:]
    scores = lax.dot_general(
        queries, keys_here, (((1,), (1,)), ((), ())), preferred_element_type=jnp.float32
    )
    scores = scores * HD ** (-0.5) - cum_gate[0, 0][None, :]
    row_top = jnp.max(scores, axis=1)
    weights = jnp.exp(scores - row_top[:, None])
    row_total = jnp.sum(weights, axis=1)
    summed = jnp.dot(weights, values_here.astype(jnp.float32), precision=lax.Precision.HIGHEST)
    out_full = lax.dynamic_update_slice(
        jnp.zeros((seq_count, query_heads, HD), jnp.float32),
        summed[None],
        (seq_index, head_index * group_size, 0),
    )
    top_full = lax.dynamic_update_slice(
        jnp.full((seq_count, query_heads), SCORE_FLOOR, jnp.float32),
        row_top[None],
        (seq_index, head_index * group_size),
    )
    sum_full = lax.dynamic_update_slice(
        jnp.zeros((seq_count, query_heads), jnp.float32),
        row_total[None],
        (seq_index, head_index * group_size),
    )
    merged_out, merged_top, merged_sum = merged_by_axis(
        (out_full, top_full, sum_full), SP_TP, combine
    )
    first_read = merged_out / merged_sum[..., None]
    return (kv_cache, first_read)


def solution(mesh):
    split = Mesh(
        mesh.devices.reshape(mesh.shape["gr"], 4, 4, 4, 2), ("gr", "sp_0", "sp_1", "tp_0", "tp_1")
    )
    return jax.shard_map(
        shards,
        mesh=split,
        in_specs=(P("gr", SP_TP, None), P(), P(), P(), P("gr", None, None), P(GR_SP, TP, None)),
        out_specs=(P(GR_SP, TP, None, None), P("gr", None, None)),
        check_vma=False,
    )
```

```python
import jax
import jax.numpy as jnp
from jax import lax
from jax.experimental import pallas as pl
from jax.experimental.pallas import tpu as pltpu
from jax.sharding import Mesh
from jax.sharding import PartitionSpec as P

HD = 64
AXES = ("z", "x", "y", "core")
SP, TP = AXES[:2], AXES[2:]
MESH = pl.DeviceIdType.MESH
NORM_FLOOR = 0.05
ROWS = 128
STEPS = 16
BURST = 5
DEPTH = 4
KV = (((1,), (1,)), ((), ()))


def across(z, kz):
    flip = z + 1 - 2 * (z % 2)
    return ((1 - kz % 2) * z + (kz % 2) * flip + 2 * (kz // 2)) % 4


def peer_of(me, kz, kx, ky, kc):
    z, x, y, c = me
    return across(z, kz), (x + kx) % 4, (y + ky) % 4, (c + kc) % 2


def step_of(i):
    j = i % 4
    return 3 - (j % 2 * 2 + j // 2), (i // 4 + j + 2) % 4


def device_of(t):
    return dict(zip(AXES, t))


def send(src, dst, send_sem, recv_sem, to):
    pltpu.make_async_remote_copy(
        src, dst, send_sem, recv_sem, device_id=device_of(to), device_id_type=MESH
    ).start()


def await_bytes(like, sem):
    pltpu.make_async_copy(like, like, sem).wait()


def merged(parts, lane):
    tops = [p[:, :1] for p in parts]
    top = tops[0]
    for t in tops[1:]:
        top = jnp.maximum(top, t)
    total = sum(jnp.exp(t - top) * p for t, p in zip(tops, parts))
    return jnp.where(lane == 0, top, total)


def kernel(
    tok_hbm, gain_hbm, wk_hbm, wv_hbm, query_hbm, gate_hbm, kv_hbm, read_hbm,
    tok, gain, wk, wv, query, padded, normed, made, gates, packed,
    part, part_in, row, row_in, final, final_in, read_in, lined, read,
    tok_sem, in_sem, wave_sem, send_sem, recv_sem,
):
    me = tuple(lax.axis_index(a) for a in AXES)
    z, x, y, core = me
    chip = z * 16 + x * 4 + y
    mine = chip * 2 + core
    sp, tp = z * 4 + x, y * 2 + core

    def tok_copy(i):
        kz, kx = step_of(i)
        rows = pl.ds(pl.multiple_of((x + kx) % 4 * ROWS, ROWS), ROWS)
        return pltpu.make_async_copy(tok_hbm.at[across(z, kz), rows], tok.at[i], tok_sem.at[i])

    in_copies = [
        pltpu.make_async_copy(src, dst, in_sem.at[n])
        for n, (src, dst) in enumerate((
            (wk_hbm, wk), (wv_hbm, wv), (gain_hbm, gain), (query_hbm, query),
            (gate_hbm.at[chip], gates.at[core * 64 + chip]),
        ))
    ]
    tok_copy(0).start()
    for copy in in_copies:
        copy.start()

    @pl.loop(1, STEPS)
    def _(i):
        tok_copy(i).start()

    barrier = pltpu.get_barrier_semaphore()

    @pl.loop(1, 128)
    def _(n):
        k = 128 - n
        to = peer_of(me, k // 32, k // 8 % 4, k // 2 % 4, k % 2)
        pl.semaphore_signal(barrier, inc=1, device_id=device_of(to), device_id_type=MESH)

    def send_step(i):
        kz, kx = step_of(i)

        @pl.loop(0, 8)
        def _(j):
            to = peer_of(me, kz, kx, j // 2, j % 2)

            @pl.when(i * 8 + j != (STEPS - 1) * 8)
            def _():
                slot = to[0] * 32 + to[1] * 8 + to[2] * 2 + to[3]
                send(made.at[slot], kv_hbm.at[mine], wave_sem.at[i], recv_sem.at[0], to)

    def await_step(i, n=8):
        await_bytes(made.at[pl.ds(0, n)], wave_sem.at[i])

    def send_gates():
        @pl.loop(1, 64)
        def _(k):
            to = peer_of(me, k // 16, k // 4 % 4, k % 4, 0)
            send(
                gate_hbm.at[to[0] * 16 + to[1] * 4 + to[2]], gates.at[core * 64 + chip],
                send_sem.at[0], recv_sem.at[1], to,
            )

    mate = (z, x, y, 1 - core)

    for copy in in_copies:
        copy.wait()

    @pl.loop(0, STEPS)
    def _(i):
        kz, kx = step_of(i)
        tok_copy(i).wait()
        for r in range(0, ROWS, 16):
            wide = tok[i, pl.ds(r, 16)].astype(jnp.float32)
            mean = jnp.sum(wide * wide, axis=-1, keepdims=True) * (1.0 / wide.shape[-1])
            scale = lax.rsqrt(mean + NORM_FLOOR)
            normed[pl.ds(r, 16)] = (wide * scale * gain[...]).astype(jnp.bfloat16)

        keys = jnp.dot(normed[...], wk[...], preferred_element_type=jnp.float32)
        values = jnp.dot(normed[...], wv[...], preferred_element_type=jnp.float32)
        base = across(z, kz) * 32 + (x + kx) % 4 * 8
        for h in range(4):
            cols = slice(h * HD, (h + 1) * HD)
            both = jnp.concatenate([keys[:, cols], values[:, cols]], axis=1).astype(jnp.bfloat16)
            made[base + 2 * h] = both[:64]
            made[base + 2 * h + 1] = both[64:]

        @pl.when(i == 0)
        def _():
            pl.semaphore_wait(barrier, 127)

        @pl.when(i < BURST)
        def _():
            send_step(i)

        @pl.when(i == 0)
        def _():
            send_gates()

        @pl.when(i == 8)
        def _():
            await_bytes(gates.at[pl.ds(0, 63)], recv_sem.at[1])
            held = gates.at[pl.ds(core * 64, 64)]
            send(held, held, send_sem.at[1], recv_sem.at[2], mate)

    own = pltpu.make_async_copy(made.at[mine], kv_hbm.at[mine], in_sem.at[0])
    own.start()

    lane = lax.broadcasted_iota(jnp.int32, (8, 2 * HD), 1)
    lane16 = lax.broadcasted_iota(jnp.int32, (16, 2 * HD), 1)
    for g in range(4):
        wide = query[g].astype(jnp.float32)
        both = jnp.concatenate([wide, jnp.zeros_like(wide)], axis=1)
        for h in range(4):
            padded[g * 4 + h] = both[h * 8 : (h + 1) * 8]

    await_bytes(gates.at[pl.ds(0, 64)], recv_sem.at[2])

    @pl.loop(0, 4)
    def _(g):
        for h in range(4):
            for c in range(4):
                for b in range(2):
                    packed[b, h * 4 + c : h * 4 + c + 1] = gates[b * 64 + g * 16 + c * 4 + h]
        low, high = packed[0], packed[1]
        low_turned, high_turned = (
            jnp.concatenate([t[:, HD:], t[:, :HD]], axis=1) for t in (low, high)
        )
        gate = jnp.where(
            lane16 < HD,
            jnp.where(core == 0, low, low_turned),
            jnp.where(core == 0, high_turned, high),
        )
        for h in range(4):
            q = padded[g * 4 + h].astype(jnp.bfloat16)
            pieces = [
                made[pl.ds(g * 32 + c * 8 + h * 2, 2)].reshape(ROWS, 2 * HD) for c in range(4)
            ]
            score = jnp.concatenate(
                [
                    lax.dot_general(q, p, KV, preferred_element_type=jnp.float32) * HD ** (-0.5)
                    - gate[h * 4 + c : h * 4 + c + 1]
                    for c, p in enumerate(pieces)
                ],
                axis=1,
            )
            top = jnp.max(score, axis=1, keepdims=True)
            weight = jnp.exp(score - top)
            total = jnp.sum(weight, axis=1, keepdims=True)
            first = weight.astype(jnp.bfloat16).astype(jnp.float32)
            second = (weight - first).astype(jnp.bfloat16).astype(jnp.float32)
            third = weight - first - second
            split = jnp.concatenate([first, second, third], axis=0).astype(jnp.bfloat16)
            out = jnp.dot(
                split, jnp.concatenate(pieces, axis=0), preferred_element_type=jnp.float32
            )
            out = out[:8] + out[8:16] + out[16:]
            part[g * 4 + h] = jnp.where(lane == 0, top, jnp.where(lane < HD, total, out))

    def send_part():
        @pl.loop(1, 8)
        def _(k):
            to = peer_of(me, 0, 0, k // 2, k % 2)
            send(
                part.at[pl.ds((to[2] * 2 + to[3]) * 2, 2)], part_in.at[pl.ds(tp * 2, 2)],
                send_sem.at[2], recv_sem.at[3], to,
            )

    def send_row():
        await_bytes(part_in.at[pl.ds(0, 14)], recv_sem.at[3])
        for n in range(2):
            part_in[tp * 2 + n] = part[tp * 2 + n]
        for n in range(2):
            one = merged([part_in[t * 2 + n] for t in range(8)], lane)
            for j in range(8):
                row[n * 8 + j] = one[j : j + 1]

        @pl.loop(1, 16)
        def _(k):
            to = peer_of(me, k // 4, k % 4, 0, 0)
            send(row.at[to[0] * 4 + to[1]], row_in.at[sp], send_sem.at[3], recv_sem.at[4], to)

    def send_final():
        await_bytes(row_in.at[pl.ds(0, 15)], recv_sem.at[4])
        row_in[sp] = row[sp]
        one = merged([row_in[s] for s in range(16)], lane[:1])
        done = one / one[:, 1:2]
        final[0] = done
        final_in[sp] = done

        @pl.loop(1, 16)
        def _(k):
            to = peer_of(me, k // 4, k % 4, 0, 0)
            send(final.at[0], final_in.at[sp], send_sem.at[4], recv_sem.at[5], to)

    def send_read():
        await_bytes(final_in.at[pl.ds(0, 15)], recv_sem.at[5])
        for s in range(16):
            read_in[tp, s] = final_in[s]

        @pl.loop(1, 8)
        def _(k):
            to = peer_of(me, 0, 0, k // 2, k % 2)
            send(final_in, read_in.at[tp], send_sem.at[5], recv_sem.at[6], to)

    send_part()

    @pl.loop(BURST, STEPS)
    def _(i):
        await_step(i - DEPTH)
        send_step(i)
        pl.when(i == 7)(send_row)
        pl.when(i == 9)(send_final)
        pl.when(i == 11)(send_read)

    await_bytes(read_in.at[pl.ds(0, 7)], recv_sem.at[6])
    for t in range(8):
        for s in range(16):
            lined[s : s + 1] = read_in[t, s]
        read[t // 2, t % 2 * 16 : t % 2 * 16 + 16] = lined[...][:, HD:]
    out_copy = pltpu.make_async_copy(read, read_hbm, in_sem.at[1])
    out_copy.start()

    await_step(0)
    for i in range(STEPS - DEPTH, STEPS):
        await_step(i, 7 if i == STEPS - 1 else 8)
    await_bytes(gates.at[pl.ds(0, 63)], send_sem.at[0])
    await_bytes(gates.at[pl.ds(0, 64)], send_sem.at[1])
    await_bytes(part_in.at[pl.ds(0, 14)], send_sem.at[2])
    await_bytes(row_in.at[pl.ds(0, 15)], send_sem.at[3])
    await_bytes(final_in.at[pl.ds(0, 15)], send_sem.at[4])
    await_bytes(read_in.at[pl.ds(0, 7)], send_sem.at[5])
    own.wait()
    out_copy.wait()
    pltpu.make_async_copy(made.at[pl.ds(0, 127)], kv_hbm.at[pl.ds(0, 127)], recv_sem.at[0]).wait()


def shards(tokens, norm_gain, w_key, w_value, new_query, cum_gate):
    width = tokens.shape[-1]
    lanes = 2 * HD
    bf16, f32 = jnp.bfloat16, jnp.float32
    kv_cache, first_read = pl.pallas_call(
        kernel,
        out_shape=[
            jax.ShapeDtypeStruct((128, 64, lanes), bf16),
            jax.ShapeDtypeStruct(new_query.shape, f32),
        ],
        in_specs=[pl.BlockSpec(memory_space=pl.ANY)] * 6,
        out_specs=[pl.BlockSpec(memory_space=pl.ANY)] * 2,
        scratch_shapes=[
            pltpu.VMEM((STEPS, ROWS, width), bf16),
            pltpu.VMEM((1, width), f32),
            pltpu.VMEM(w_key.shape, bf16),
            pltpu.VMEM(w_value.shape, bf16),
            pltpu.VMEM(new_query.shape, bf16),
            pltpu.VMEM((16, 8, lanes), f32),
            pltpu.VMEM((ROWS, width), bf16),
            pltpu.VMEM((128, 64, lanes), bf16),
            pltpu.VMEM((128, 1, lanes), f32),
            pltpu.VMEM((2, 16, lanes), f32),
            pltpu.VMEM((16, 8, lanes), f32),
            pltpu.VMEM((16, 8, lanes), f32),
            pltpu.VMEM((16, 1, lanes), f32),
            pltpu.VMEM((16, 1, lanes), f32),
            pltpu.VMEM((1, 1, lanes), f32),
            pltpu.VMEM((16, 1, lanes), f32),
            pltpu.VMEM((8, 16, 1, lanes), f32),
            pltpu.VMEM((16, lanes), f32),
            pltpu.VMEM(new_query.shape, f32),
            pltpu.SemaphoreType.DMA((STEPS,)),
            pltpu.SemaphoreType.DMA((5,)),
            pltpu.SemaphoreType.DMA((STEPS,)),
            pltpu.SemaphoreType.DMA((6,)),
            pltpu.SemaphoreType.DMA((7,)),
        ],
        compiler_params=pltpu.CompilerParams(collective_id=0, has_side_effects=True),
    )(
        tokens, norm_gain.reshape(1, width), w_key, w_value, new_query,
        cum_gate.reshape(64, 1, lanes),
    )
    return kv_cache.reshape(1, 1, 128 * 64, lanes), first_read


def solution(mesh):
    split = Mesh(mesh.devices.reshape(mesh.shape["gr"], 4, 4, 4, 2), ("gr", *AXES))
    return jax.shard_map(
        shards,
        mesh=split,
        in_specs=(
            P("gr", (*SP, *TP), None), P(), P(), P(), P("gr", None, None), P(("gr", *SP), TP, None)
        ),
        out_specs=(P(("gr", *SP), TP, None, None), P("gr", None, None)),
        check_vma=False,
    )
```

```python
import jax
import jax.numpy as jnp
from jax import lax
from jax.experimental import pallas as pl
from jax.experimental.pallas import tpu as pltpu
from jax.sharding import Mesh
from jax.sharding import PartitionSpec as P

HD = 64
AXES = ("z", "x", "y", "core")
SP, TP = AXES[:2], AXES[2:]
MESH = pl.DeviceIdType.MESH
NORM_FLOOR = 0.05
ROWS = 128
STEPS = 16
BURST = 8
DEPTH = 4
KV = (((1,), (1,)), ((), ()))


def across(z, kz):
    flip = z + 1 - 2 * (z % 2)
    return ((1 - kz % 2) * z + (kz % 2) * flip + 2 * (kz // 2)) % 4


def step_of(i):
    j = i % 4
    return 3 - (j % 2 * 2 + j // 2), (i // 4 + j + 2) % 4


def device_of(t):
    return dict(zip(AXES, t))


def send(src, dst, send_sem, recv_sem, to):
    pltpu.make_async_remote_copy(
        src, dst, send_sem, recv_sem, device_id=device_of(to), device_id_type=MESH
    ).start()


def await_bytes(like, sem):
    pltpu.make_async_copy(like, like, sem).wait()


def merged(parts, lane):
    tops = [p[:, :1] for p in parts]
    top = tops[0]
    for t in tops[1:]:
        top = jnp.maximum(top, t)
    total = sum(jnp.exp(t - top) * p for t, p in zip(tops, parts))
    return jnp.where(lane == 0, top, total)


def kernel(
    tok_hbm, gain_hbm, wk_hbm, wv_hbm, query_hbm, gate_hbm, cache, read,
    tok, gain, wk, wv, query, padded, normed, made, gates, packed,
    part, part_in, row, row_in, final, final_in, read_in, lined,
    tok_sem, in_sem, wave_sem, send_sem, recv_sem,
):
    me = tuple(lax.axis_index(a) for a in AXES)
    z, x, y, core = me
    chip = z * 16 + x * 4 + y
    mine = chip * 2 + core
    sp, tp = z * 4 + x, y * 2 + core

    zs = [across(z, k) for k in range(4)]
    xs = [(x + k) % 4 for k in range(4)]
    ys = [(y + k) % 4 for k in range(4)]
    cores = [core, 1 - core]
    tps = [(yt, ct) for yt in ys for ct in cores]
    sps = [(zt, xt) for zt in zs for xt in xs]

    def tok_copy(i):
        kz, kx = step_of(i)
        rows = pl.ds(pl.multiple_of((x + kx) % 4 * ROWS, ROWS), ROWS)
        return pltpu.make_async_copy(tok_hbm.at[across(z, kz), rows], tok.at[i], tok_sem.at[i])

    def in_copy(n, src, dst):
        return pltpu.make_async_copy(src, dst, in_sem.at[n])

    early = [in_copy(0, wk_hbm, wk), in_copy(1, wv_hbm, wv), in_copy(2, gain_hbm, gain)]
    late = [
        in_copy(3, query_hbm, query), in_copy(4, gate_hbm.at[chip], gates.at[core * 64 + chip])
    ]
    tok_copy(0).start()
    for copy in early:
        copy.start()
    tok_copy(1).start()

    barrier = pltpu.get_barrier_semaphore()
    with jax.named_scope("signals"):
        for zt in zs[::-1]:
            for xt in xs[::-1]:
                for yt, ct in tps[::-1]:
                    if zt is not zs[0] or xt is not xs[0] or yt is not ys[0] or ct is not core:
                        pl.semaphore_signal(
                            barrier, inc=1, device_id=device_of((zt, xt, yt, ct)), device_id_type=MESH
                        )

    def send_step(i):
        kz, kx = step_of(i)
        zt, xt = across(z, kz), (x + kx) % 4
        base = zt * 32 + xt * 8
        for j, (yt, ct) in enumerate(tps):

            def one():
                send(
                    made.at[base + yt * 2 + ct], cache.at[mine], wave_sem.at[i], recv_sem.at[0],
                    (zt, xt, yt, ct),
                )

            if j:
                one()
            else:
                pl.when(i != STEPS - 1)(one)

    def await_step(i, n=8):
        await_bytes(made.at[pl.ds(0, n)], wave_sem.at[i])

    def send_gates():
        for zt, xt in sps:
            for yt in ys:
                if zt is not zs[0] or xt is not xs[0] or yt is not ys[0]:
                    send(
                        gate_hbm.at[zt * 16 + xt * 4 + yt], gates.at[core * 64 + chip],
                        send_sem.at[0], recv_sem.at[1], (zt, xt, yt, core),
                    )

    def project(i, n):
        for s in range(n):
            with jax.named_scope("tokwait"):
                tok_copy(i + s).wait()
        with jax.named_scope("norm"):
            for r in range(0, n * ROWS, 16):
                wide = tok[i + r // ROWS, pl.ds(r % ROWS, 16)].astype(jnp.float32)
                mean = jnp.sum(wide * wide, axis=-1, keepdims=True) * (1.0 / wide.shape[-1])
                scale = lax.rsqrt(mean + NORM_FLOOR)
                normed[pl.ds(r, 16)] = (wide * scale * gain[...]).astype(jnp.bfloat16)

        with jax.named_scope("dots"):
            lhs = normed[pl.ds(0, n * ROWS)]
            keys = jnp.dot(lhs, wk[...], preferred_element_type=jnp.float32)
            values = jnp.dot(lhs, wv[...], preferred_element_type=jnp.float32)
            for s in range(n):
                kz, kx = step_of(i + s)
                base = across(z, kz) * 32 + (x + kx) % 4 * 8
                rows = slice(s * ROWS, (s + 1) * ROWS)
                for h in range(4):
                    cols = slice(h * HD, (h + 1) * HD)
                    both = jnp.concatenate([keys[rows, cols], values[rows, cols]], axis=1)
                    both = both.astype(jnp.bfloat16)
                    made[base + 2 * h] = both[:64]
                    made[base + 2 * h + 1] = both[64:]

    mate = (z, x, y, 1 - core)

    with jax.named_scope("inputs"):
        for copy in early:
            copy.wait()
    for i in range(2, 4):
        tok_copy(i).start()
    project(0, 1)
    with jax.named_scope("barrier"):
        pl.semaphore_wait(barrier, 127)
    with jax.named_scope("sendstep"):
        send_step(0)
    with jax.named_scope("sendgates"):
        send_gates()
    for copy in late:
        copy.start()
    for i in range(4, 6):
        tok_copy(i).start()
    project(1, 1)
    send_step(1)

    @pl.loop(2, STEPS, step=2)
    def _(i):
        @pl.when(i < STEPS - 4)
        def _():
            for n in range(4, 6):
                tok_copy(i + n).start()

        project(i, 2)

        @pl.when(i < BURST)
        def _():
            send_step(i)
            send_step(i + 1)

        @pl.when(i == 10)
        def _():
            with jax.named_scope("waitgates"):
                late[1].wait()
                await_bytes(gates.at[pl.ds(0, 63)], recv_sem.at[1])
            held = gates.at[pl.ds(core * 64, 64)]
            send(held, held, send_sem.at[1], recv_sem.at[2], mate)

    late[0].wait()
    with jax.named_scope("selfpiece"):
        cache[mine] = made[mine]

    lane = lax.broadcasted_iota(jnp.int32, (8, 2 * HD), 1)
    lane16 = lax.broadcasted_iota(jnp.int32, (16, 2 * HD), 1)
    for g in range(4):
        wide = query[g].astype(jnp.float32)
        both = jnp.concatenate([wide, jnp.zeros_like(wide)], axis=1)
        for h in range(4):
            padded[g * 4 + h] = both[h * 8 : (h + 1) * 8]

    with jax.named_scope("gatewait"):
        await_bytes(gates.at[pl.ds(0, 64)], recv_sem.at[2])

    with jax.named_scope("attention"):

        @pl.loop(0, 4)
        def _(g):
            for h in range(4):
                for c in range(4):
                    for b in range(2):
                        packed[b, h * 4 + c : h * 4 + c + 1] = gates[b * 64 + g * 16 + c * 4 + h]
            low, high = packed[0], packed[1]
            low_turned, high_turned = (
                jnp.concatenate([t[:, HD:], t[:, :HD]], axis=1) for t in (low, high)
            )
            gate = jnp.where(
                lane16 < HD,
                jnp.where(core == 0, low, low_turned),
                jnp.where(core == 0, high_turned, high),
            )
            for h in range(4):
                q = padded[g * 4 + h].astype(jnp.bfloat16)
                pieces = [
                    made[pl.ds(g * 32 + c * 8 + h * 2, 2)].reshape(ROWS, 2 * HD) for c in range(4)
                ]
                score = jnp.concatenate(
                    [
                        lax.dot_general(q, p, KV, preferred_element_type=jnp.float32) * HD ** (-0.5)
                        - gate[h * 4 + c : h * 4 + c + 1]
                        for c, p in enumerate(pieces)
                    ],
                    axis=1,
                )
                top = jnp.max(score, axis=1, keepdims=True)
                weight = jnp.exp(score - top)
                total = jnp.sum(weight, axis=1, keepdims=True)
                first = weight.astype(jnp.bfloat16).astype(jnp.float32)
                second = (weight - first).astype(jnp.bfloat16).astype(jnp.float32)
                third = weight - first - second
                split = jnp.concatenate([first, second, third], axis=0).astype(jnp.bfloat16)
                out = jnp.dot(
                    split, jnp.concatenate(pieces, axis=0), preferred_element_type=jnp.float32
                )
                out = out[:8] + out[8:16] + out[16:]
                part[g * 4 + h] = jnp.where(lane == 0, top, jnp.where(lane < HD, total, out))

    def send_part():
        for yt, ct in tps[1:]:
            send(
                part.at[pl.ds((yt * 2 + ct) * 2, 2)], part_in.at[pl.ds(tp * 2, 2)],
                send_sem.at[2], recv_sem.at[3], (z, x, yt, ct),
            )

    def send_row():
        with jax.named_scope("wait_part"):
            await_bytes(part_in.at[pl.ds(0, 14)], recv_sem.at[3])
        for n in range(2):
            part_in[tp * 2 + n] = part[tp * 2 + n]
        for n in range(2):
            one = merged([part_in[t * 2 + n] for t in range(8)], lane)
            for j in range(8):
                row[n * 8 + j] = one[j : j + 1]

        for zt, xt in sps[1:]:
            send(
                row.at[zt * 4 + xt], row_in.at[sp], send_sem.at[3], recv_sem.at[4],
                (zt, xt, y, core),
            )

    def send_final():
        with jax.named_scope("wait_row"):
            await_bytes(row_in.at[pl.ds(0, 15)], recv_sem.at[4])
        row_in[sp] = row[sp]
        one = merged([row_in[s] for s in range(16)], lane[:1])
        done = one / one[:, 1:2]
        final[0] = done
        final_in[sp] = done

        for zt, xt in sps[1:]:
            send(
                final.at[0], final_in.at[sp], send_sem.at[4], recv_sem.at[5], (zt, xt, y, core)
            )

    def send_read():
        with jax.named_scope("wait_final"):
            await_bytes(final_in.at[pl.ds(0, 15)], recv_sem.at[5])
        for s in range(16):
            read_in[tp, s] = final_in[s]

        for yt, ct in tps[1:]:
            send(final_in, read_in.at[tp], send_sem.at[5], recv_sem.at[6], (z, x, yt, ct))

    send_part()

    @pl.loop(BURST, STEPS)
    def _(i):
        with jax.named_scope("pace"):
            await_step(i - DEPTH)
        send_step(i)
        pl.when(i == 8)(send_row)
        pl.when(i == 10)(send_final)
        pl.when(i == 12)(send_read)

    with jax.named_scope("wait_read"):
        await_bytes(read_in.at[pl.ds(0, 7)], recv_sem.at[6])
    for t in range(8):
        for s in range(16):
            lined[s : s + 1] = read_in[t, s]
        read[t // 2, t % 2 * 16 : t % 2 * 16 + 16] = lined[...][:, HD:]

    with jax.named_scope("wait_sent"):
        for i in (*range(BURST - DEPTH), *range(STEPS - DEPTH, STEPS)):
            await_step(i, 7 if i == STEPS - 1 else 8)
    await_bytes(gates.at[pl.ds(0, 63)], send_sem.at[0])
    await_bytes(gates.at[pl.ds(0, 64)], send_sem.at[1])
    await_bytes(part_in.at[pl.ds(0, 14)], send_sem.at[2])
    await_bytes(row_in.at[pl.ds(0, 15)], send_sem.at[3])
    await_bytes(final_in.at[pl.ds(0, 15)], send_sem.at[4])
    await_bytes(read_in.at[pl.ds(0, 7)], send_sem.at[5])
    with jax.named_scope("wait_all"):
        await_bytes(cache.at[pl.ds(0, 127)], recv_sem.at[0])


def shards(tokens, norm_gain, w_key, w_value, new_query, cum_gate):
    width = tokens.shape[-1]
    lanes = 2 * HD
    bf16, f32 = jnp.bfloat16, jnp.float32
    kv_cache, first_read = pl.pallas_call(
        kernel,
        out_shape=[
            pltpu.VMEM((128, 64, lanes), bf16),
            pltpu.VMEM(new_query.shape, f32),
        ],
        in_specs=[pl.BlockSpec(memory_space=pl.ANY)] * 6,
        out_specs=[pl.BlockSpec(memory_space=pltpu.VMEM)] * 2,
        scratch_shapes=[
            pltpu.VMEM((STEPS, ROWS, width), bf16),
            pltpu.VMEM((1, width), f32),
            pltpu.VMEM(w_key.shape, bf16),
            pltpu.VMEM(w_value.shape, bf16),
            pltpu.VMEM(new_query.shape, bf16),
            pltpu.VMEM((16, 8, lanes), f32),
            pltpu.VMEM((2 * ROWS, width), bf16),
            pltpu.VMEM((128, 64, lanes), bf16),
            pltpu.VMEM((128, 1, lanes), f32),
            pltpu.VMEM((2, 16, lanes), f32),
            pltpu.VMEM((16, 8, lanes), f32),
            pltpu.VMEM((16, 8, lanes), f32),
            pltpu.VMEM((16, 1, lanes), f32),
            pltpu.VMEM((16, 1, lanes), f32),
            pltpu.VMEM((1, 1, lanes), f32),
            pltpu.VMEM((16, 1, lanes), f32),
            pltpu.VMEM((8, 16, 1, lanes), f32),
            pltpu.VMEM((16, lanes), f32),
            pltpu.SemaphoreType.DMA((STEPS,)),
            pltpu.SemaphoreType.DMA((5,)),
            pltpu.SemaphoreType.DMA((STEPS,)),
            pltpu.SemaphoreType.DMA((6,)),
            pltpu.SemaphoreType.DMA((7,)),
        ],
        compiler_params=pltpu.CompilerParams(collective_id=0, has_side_effects=True),
    )(
        tokens, norm_gain.reshape(1, width), w_key, w_value, new_query,
        cum_gate.reshape(64, 1, lanes),
    )
    return kv_cache.reshape(1, 1, 128 * 64, lanes), first_read


def solution(mesh):
    split = Mesh(mesh.devices.reshape(mesh.shape["gr"], 4, 4, 4, 2), ("gr", *AXES))
    return jax.shard_map(
        shards,
        mesh=split,
        in_specs=(
            P("gr", (*SP, *TP), None), P(), P(), P(), P("gr", None, None), P(("gr", *SP), TP, None)
        ),
        out_specs=(P(("gr", *SP), TP, None, None), P("gr", None, None)),
        check_vma=False,
    )
```

```python
import jax
import jax.numpy as jnp
from jax import lax
from jax.experimental import pallas as pl
from jax.experimental.pallas import tpu as pltpu
from jax.sharding import Mesh
from jax.sharding import PartitionSpec as P

HD = 64
AXES = ("z", "x", "y", "core")
SP, TP = AXES[:2], AXES[2:]
MESH = pl.DeviceIdType.MESH
NORM_FLOOR = 0.05
ROWS = 128
STEPS = 16
BURST = 6
FOLLOW = (2, 2, 4, 2)
KV = (((1,), (1,)), ((), ()))


def across(z, kz):
    flip = z + 1 - 2 * (z % 2)
    return ((1 - kz % 2) * z + (kz % 2) * flip + 2 * (kz // 2)) % 4


def step_of(z, i):
    j = i % 4
    one, two = z % 2 * (1 - z // 2), (1 - z % 2) * (z // 2)
    even = 2 + one + j // 2 * (1 - 2 * one)
    odd = 1 - two + j // 2 * (2 * two - 1)
    return even + j % 2 * (odd - even), (i // 4 + j + 2) % 4


def device_of(t):
    return dict(zip(AXES, t))


def send(src, dst, send_sem, recv_sem, to):
    pltpu.make_async_remote_copy(
        src, dst, send_sem, recv_sem, device_id=device_of(to), device_id_type=MESH
    ).start()


def await_bytes(like, sem):
    pltpu.make_async_copy(like, like, sem).wait()


def merged(parts, lane):
    tops = [p[:, :1] for p in parts]
    top = tops[0]
    for t in tops[1:]:
        top = jnp.maximum(top, t)
    total = sum(jnp.exp(t - top) * p for t, p in zip(tops, parts))
    return jnp.where(lane == 0, top, total)


def kernel(
    tok_hbm, gain_hbm, wk_hbm, wv_hbm, query_hbm, gate_hbm, cache, read,
    tok, gain, wk, wv, gate, query, spread, normed, made, gates, packed,
    part, part_in, row, row_in, final, final_in, read_in, lined,
    tok_sem, in_sem, wave_sem, send_sem, recv_sem, up_sem,
):
    me = tuple(lax.axis_index(a) for a in AXES)
    z, x, y, core = me
    chip = z * 16 + x * 4 + y
    mine = chip * 2 + core
    sp, tp = z * 4 + x, y * 2 + core

    zs = [across(z, k) for k in range(4)]
    xs = [(x + k) % 4 for k in range(4)]
    ys = [(y + k) % 4 for k in range(4)]
    cores = [core, 1 - core]
    tps = [(yt, ct) for yt in ys for ct in cores]
    sps = [(zt, xt) for zt in zs for xt in xs]

    def tok_copy(i):
        kz, kx = step_of(z, i)
        rows = pl.ds(pl.multiple_of((x + kx) % 4 * ROWS, ROWS), ROWS)
        return pltpu.make_async_copy(tok_hbm.at[across(z, kz), rows], tok.at[i], tok_sem.at[i % 6])

    def in_copy(n, src, dst):
        return pltpu.make_async_copy(src, dst, in_sem.at[n])

    early = [
        in_copy(0, wk_hbm, wk), in_copy(1, wv_hbm, wv), in_copy(2, gain_hbm, gain),
        in_copy(3, gate_hbm, gate),
    ]
    late = in_copy(4, query_hbm, query)
    tok_copy(0).start()
    for copy in early:
        copy.start()
    tok_copy(1).start()

    barrier = pltpu.get_barrier_semaphore()
    last = len(zs) - 1
    apart = 1 - lax.axis_index("gr")
    is_last = z // last * apart

    @pl.when(is_last == 0)
    def _():
        with jax.named_scope("signals"):
            for zt in zs[::-1]:
                for xt in xs[::-1]:
                    for yt, ct in tps[::-1]:
                        if zt is not zs[0] or xt is not xs[0] or yt is not ys[0] or ct is not core:
                            pl.semaphore_signal(
                                barrier, inc=1, device_id=device_of((zt, xt, yt, ct)), device_id_type=MESH
                            )

    def await_entry():
        pl.semaphore_wait(barrier, 127 - 32 * apart + is_last)

        @pl.when(is_last == 1)
        def _():
            for zt in zs[:0:-1]:
                for xt in xs[::-1]:
                    for yt, ct in tps[::-1]:
                        pl.semaphore_signal(
                            up_sem.at[0], inc=1, device_id=device_of((zt, xt, yt, ct)), device_id_type=MESH
                        )

    def await_last():
        @pl.when((1 - is_last) * apart == 1)
        def _():
            pl.semaphore_wait(up_sem.at[0], 32)

        @pl.when(z * apart == last - 1)
        def _():
            pl.semaphore_signal(
                up_sem.at[1], inc=1, device_id=device_of((last, x, y, core)), device_id_type=MESH
            )

        @pl.when(is_last == 1)
        def _():
            pl.semaphore_wait(up_sem.at[1], 1)

    def send_steps(i, n):
        for j, (yt, ct) in enumerate(tps):
            for s in range(n):
                kz, kx = step_of(z, i + s)
                zt, xt = across(z, kz), (x + kx) % 4

                def one():
                    send(
                        made.at[zt * 32 + xt * 8 + yt * 2 + ct], cache.at[mine],
                        wave_sem.at[(i + s) % BURST], recv_sem.at[0], (zt, xt, yt, ct),
                    )

                if j:
                    one()
                else:
                    pl.when(kz + kx != 0)(one)

    def await_steps(i, n):
        for s in range(n):
            sem = wave_sem.at[(i + s) % BURST]
            kz, kx = step_of(z, i + s)
            await_bytes(made.at[pl.ds(0, 7)], sem)
            pl.when(kz + kx != 0)(lambda sem=sem: await_bytes(made.at[pl.ds(0, 1)], sem))

    def send_gates(to_last):
        for zt in zs:

            def block():
                for xt in xs:
                    for yt in ys:
                        if zt is not zs[0] or xt is not xs[0] or yt is not ys[0]:
                            send(
                                gate.at[zt * 16 + xt * 4 + yt], gates.at[core * 64 + chip],
                                send_sem.at[0], recv_sem.at[1], (zt, xt, yt, core),
                            )

            pl.when(zt // last * apart == int(to_last))(block)

    def project(i, n):
        for s in range(n):
            with jax.named_scope("tokwait"):
                tok_copy(i + s).wait()
        with jax.named_scope("norm"):
            for r in range(0, n * ROWS, 16):
                wide = tok[i + r // ROWS, pl.ds(r % ROWS, 16)].astype(jnp.float32)
                mean = jnp.sum(wide * wide, axis=-1, keepdims=True) * (1.0 / wide.shape[-1])
                scale = lax.rsqrt(mean + NORM_FLOOR)
                normed[pl.ds(r, 16)] = (wide * scale * gain[...]).astype(jnp.bfloat16)

        with jax.named_scope("dots"):
            lhs = normed[pl.ds(0, n * ROWS)]
            keys = jnp.dot(lhs, wk[...], preferred_element_type=jnp.float32)
            values = jnp.dot(lhs, wv[...], preferred_element_type=jnp.float32)
            for s in range(n):
                kz, kx = step_of(z, i + s)
                base = across(z, kz) * 32 + (x + kx) % 4 * 8
                rows = slice(s * ROWS, (s + 1) * ROWS)
                for h in range(4):
                    cols = slice(h * HD, (h + 1) * HD)
                    both = jnp.concatenate([keys[rows, cols], values[rows, cols]], axis=1)
                    both = both.astype(jnp.bfloat16)
                    made[base + 2 * h] = both[:64]
                    made[base + 2 * h + 1] = both[64:]

    mate = (z, x, y, 1 - core)

    pl.when(is_last == 1)(await_entry)
    with jax.named_scope("inputs"):
        for copy in early:
            copy.wait()
    for i in range(2, 4):
        tok_copy(i).start()
    project(0, 1)
    with jax.named_scope("barrier"):
        pl.when(is_last == 0)(await_entry)
    with jax.named_scope("sendgates"):
        send_gates(False)
    gates[core * 64 + chip] = gate[chip]
    send_steps(0, 1)
    late.start()
    for i in range(4, 6):
        tok_copy(i).start()
    project(1, 1)
    send_steps(1, 1)
    project(2, 2)
    with jax.named_scope("awaitlast"):
        await_last()
    with jax.named_scope("sendgates"):
        send_gates(True)
    send_steps(2, 2)
    for i in range(6, 8):
        tok_copy(i).start()

    @pl.loop(4, STEPS, step=2)
    def _(i):
        @pl.when(i < STEPS - 4)
        def _():
            for n in range(4, 6):
                tok_copy(i + n).start()

        project(i, 2)

        @pl.when(i < BURST)
        def _():
            send_steps(i, 2)

        @pl.when(i == 12)
        def _():
            with jax.named_scope("waitgates"):
                await_bytes(gates.at[pl.ds(0, 63)], recv_sem.at[1])
            held = gates.at[pl.ds(core * 64, 64)]
            send(held, held, send_sem.at[1], recv_sem.at[2], mate)

    late.wait()
    with jax.named_scope("selfpiece"):
        cache[mine] = made[mine]

    lane = lax.broadcasted_iota(jnp.int32, (8, 2 * HD), 1)
    lane16 = lax.broadcasted_iota(jnp.int32, (16, 2 * HD), 1)
    for g in range(4):
        wide = query[g].astype(jnp.float32)
        spread[g] = jnp.zeros(spread.shape[1:], jnp.float32)
        for h in range(4):
            spread[g, h * 8 : (h + 1) * 8, h * 2 * HD : h * 2 * HD + HD] = wide[h * 8 : (h + 1) * 8]

    with jax.named_scope("gatewait"):
        await_bytes(gates.at[pl.ds(0, 64)], recv_sem.at[2])

    with jax.named_scope("attention"):

        @pl.loop(0, 4)
        def _(g):
            for h in range(4):
                for c in range(4):
                    for b in range(2):
                        packed[b, h * 4 + c : h * 4 + c + 1] = gates[b * 64 + g * 16 + c * 4 + h]
            low, high = packed[0], packed[1]
            low_turned, high_turned = (
                jnp.concatenate([t[:, HD:], t[:, :HD]], axis=1) for t in (low, high)
            )
            bias = jnp.where(
                lane16 < HD,
                jnp.where(core == 0, low, low_turned),
                jnp.where(core == 0, high_turned, high),
            )
            pairs = jnp.concatenate(
                [
                    jnp.concatenate(
                        [
                            made[pl.ds(g * 32 + c * 8 + h * 2, 2)].reshape(ROWS, 2 * HD)
                            for h in range(4)
                        ],
                        axis=1,
                    )
                    for c in range(4)
                ],
                axis=0,
            )
            away = jnp.concatenate(
                [
                    jnp.broadcast_to(
                        jnp.concatenate(
                            [bias[h * 4 + c : h * 4 + c + 1] for c in range(4)], axis=1
                        ),
                        (8, 4 * ROWS),
                    )
                    for h in range(4)
                ],
                axis=0,
            )
            score = lax.dot_general(
                spread[g].astype(jnp.bfloat16), pairs, KV, preferred_element_type=jnp.float32
            )
            score = score * HD ** (-0.5) - away
            top = jnp.max(score, axis=1, keepdims=True)
            weight = jnp.exp(score - top)
            total = jnp.sum(weight, axis=1, keepdims=True)
            first = weight.astype(jnp.bfloat16).astype(jnp.float32)
            second = (weight - first).astype(jnp.bfloat16).astype(jnp.float32)
            third = weight - first - second
            split = jnp.concatenate([first, second, third], axis=0).astype(jnp.bfloat16)
            out = jnp.dot(split, pairs, preferred_element_type=jnp.float32)
            out = out[:32] + out[32:64] + out[64:]
            for h in range(4):
                rows = slice(h * 8, (h + 1) * 8)
                part[g * 4 + h] = jnp.where(
                    lane == 0,
                    top[rows],
                    jnp.where(lane < HD, total[rows], out[rows, h * 2 * HD : (h + 1) * 2 * HD]),
                )

    def send_part():
        for yt, ct in tps[1:]:
            send(
                part.at[pl.ds((yt * 2 + ct) * 2, 2)], part_in.at[pl.ds(tp * 2, 2)],
                send_sem.at[2], recv_sem.at[3], (z, x, yt, ct),
            )

    def send_row():
        with jax.named_scope("wait_part"):
            await_bytes(part_in.at[pl.ds(0, 14)], recv_sem.at[3])
        for n in range(2):
            part_in[tp * 2 + n] = part[tp * 2 + n]
        for n in range(2):
            one = merged([part_in[t * 2 + n] for t in range(8)], lane)
            for j in range(8):
                row[n * 8 + j] = one[j : j + 1]

        for zt, xt in sps[1:]:
            send(
                row.at[zt * 4 + xt], row_in.at[sp], send_sem.at[3], recv_sem.at[4],
                (zt, xt, y, core),
            )

    def send_final():
        with jax.named_scope("wait_row"):
            await_bytes(row_in.at[pl.ds(0, 15)], recv_sem.at[4])
        row_in[sp] = row[sp]
        one = merged([row_in[s] for s in range(16)], lane[:1])
        done = one / one[:, 1:2]
        final[0] = done
        final_in[sp] = done

        for zt, xt in sps[1:]:
            send(
                final.at[0], final_in.at[sp], send_sem.at[4], recv_sem.at[5], (zt, xt, y, core)
            )

    def send_read():
        with jax.named_scope("wait_final"):
            await_bytes(final_in.at[pl.ds(0, 15)], recv_sem.at[5])
        for s in range(16):
            read_in[tp, s] = final_in[s]

        for yt, ct in tps[1:]:
            send(final_in, read_in.at[tp], send_sem.at[5], recv_sem.at[6], (z, x, yt, ct))

    at = BURST
    for stage, n in zip((send_part, send_row, send_final, send_read), FOLLOW):
        stage()
        if n:
            with jax.named_scope("pace"):
                await_steps(at - BURST, n)
            send_steps(at, n)
        at += n

    with jax.named_scope("wait_read"):
        await_bytes(read_in.at[pl.ds(0, 7)], recv_sem.at[6])
    for t in range(8):
        for s in range(16):
            lined[s : s + 1] = read_in[t, s]
        read[t // 2, t % 2 * 16 : t % 2 * 16 + 16] = lined[...][:, HD:]

    with jax.named_scope("wait_sent"):
        await_steps(STEPS - BURST, BURST)
    await_bytes(gates.at[pl.ds(0, 63)], send_sem.at[0])
    await_bytes(gates.at[pl.ds(0, 64)], send_sem.at[1])
    await_bytes(part_in.at[pl.ds(0, 14)], send_sem.at[2])
    await_bytes(row_in.at[pl.ds(0, 15)], send_sem.at[3])
    await_bytes(final_in.at[pl.ds(0, 15)], send_sem.at[4])
    await_bytes(read_in.at[pl.ds(0, 7)], send_sem.at[5])
    with jax.named_scope("wait_all"):
        await_bytes(cache.at[pl.ds(0, 127)], recv_sem.at[0])


def store_kernel(cache, read, cache_out, read_out, sem):
    copies = [pltpu.make_async_copy(read, read_out, sem.at[4])] + [
        pltpu.make_async_copy(cache.at[pl.ds(n * 32, 32)], cache_out.at[pl.ds(n * 32, 32)], sem.at[n])
        for n in range(4)
    ]
    for copy in copies:
        copy.start()
    for copy in copies:
        copy.wait()


def shards(tokens, norm_gain, w_key, w_value, new_query, cum_gate):
    width = tokens.shape[-1]
    lanes = 2 * HD
    bf16, f32 = jnp.bfloat16, jnp.float32
    cache, read = pl.pallas_call(
        kernel,
        out_shape=[
            pltpu.VMEM((128, 64, lanes), bf16),
            pltpu.VMEM(new_query.shape, f32),
        ],
        in_specs=[pl.BlockSpec(memory_space=pl.ANY)] * 6,
        out_specs=[pl.BlockSpec(memory_space=pltpu.VMEM)] * 2,
        scratch_shapes=[
            pltpu.VMEM((STEPS, ROWS, width), bf16),
            pltpu.VMEM((1, width), f32),
            pltpu.VMEM(w_key.shape, bf16),
            pltpu.VMEM(w_value.shape, bf16),
            pltpu.VMEM((64, 1, lanes), f32),
            pltpu.VMEM(new_query.shape, bf16),
            pltpu.VMEM((4, 32, 4 * lanes), f32),
            pltpu.VMEM((2 * ROWS, width), bf16),
            pltpu.VMEM((128, 64, lanes), bf16),
            pltpu.VMEM((128, 1, lanes), f32),
            pltpu.VMEM((2, 16, lanes), f32),
            pltpu.VMEM((16, 8, lanes), f32),
            pltpu.VMEM((16, 8, lanes), f32),
            pltpu.VMEM((16, 1, lanes), f32),
            pltpu.VMEM((16, 1, lanes), f32),
            pltpu.VMEM((1, 1, lanes), f32),
            pltpu.VMEM((16, 1, lanes), f32),
            pltpu.VMEM((8, 16, 1, lanes), f32),
            pltpu.VMEM((16, lanes), f32),
            pltpu.SemaphoreType.DMA((6,)),
            pltpu.SemaphoreType.DMA((5,)),
            pltpu.SemaphoreType.DMA((BURST,)),
            pltpu.SemaphoreType.DMA((6,)),
            pltpu.SemaphoreType.DMA((7,)),
            pltpu.SemaphoreType.REGULAR((2,)),
        ],
        compiler_params=pltpu.CompilerParams(collective_id=0, has_side_effects=True),
    )(
        tokens, norm_gain.reshape(1, width), w_key, w_value, new_query,
        cum_gate.reshape(64, 1, lanes),
    )
    cache = pltpu.with_memory_space_constraint(cache, pltpu.VMEM)
    read = pltpu.with_memory_space_constraint(read, pltpu.VMEM)
    kv_cache, first_read = pl.pallas_call(
        store_kernel,
        out_shape=[
            jax.ShapeDtypeStruct(cache.shape, bf16), jax.ShapeDtypeStruct(read.shape, f32)
        ],
        in_specs=[pl.BlockSpec(memory_space=pltpu.VMEM)] * 2,
        out_specs=[pl.BlockSpec(memory_space=pl.ANY)] * 2,
        scratch_shapes=[pltpu.SemaphoreType.DMA((5,))],
    )(cache, read)
    return kv_cache.reshape(1, 1, 128 * 64, lanes), first_read


def solution(mesh):
    split = Mesh(mesh.devices.reshape(mesh.shape["gr"], 4, 4, 4, 2), ("gr", *AXES))
    return jax.shard_map(
        shards,
        mesh=split,
        in_specs=(
            P("gr", (*SP, *TP), None), P(), P(), P(), P("gr", None, None), P(("gr", *SP), TP, None)
        ),
        out_specs=(P(("gr", *SP), TP, None, None), P("gr", None, None)),
        check_vma=False,
    )
```

```python
import jax
import jax.numpy as jnp
from jax import lax
from jax.experimental import pallas as pl
from jax.experimental.pallas import tpu as pltpu
from jax.sharding import Mesh
from jax.sharding import PartitionSpec as P

HD = 64
AXES = ("z", "x", "y", "core")
SP, TP = AXES[:2], AXES[2:]
MESH = pl.DeviceIdType.MESH
NORM_FLOOR = 0.05
ROWS = 128
STEPS = 16
BURST = 6
FOLLOW = (2, 2, 4, 2)
KV = (((1,), (1,)), ((), ()))


def across(z, kz):
    flip = z + 1 - 2 * (z % 2)
    return ((1 - kz % 2) * z + (kz % 2) * flip + 2 * (kz // 2)) % 4


def step_of(z, apart, i):
    j = i % 4
    one, two = z % 2 * (1 - z // 2) * apart + 1 - apart, (1 - z % 2) * (z // 2) * apart
    even = 2 + one + j // 2 * (1 - 2 * one)
    odd = 1 - two + j // 2 * (2 * two - 1)
    return even + j % 2 * (odd - even), (i // 4 + j + 2) % 4


def device_of(t):
    return dict(zip(AXES, t))


def send(src, dst, send_sem, recv_sem, to):
    pltpu.make_async_remote_copy(
        src, dst, send_sem, recv_sem, device_id=device_of(to), device_id_type=MESH
    ).start()


def await_bytes(like, sem):
    pltpu.make_async_copy(like, like, sem).wait()


def merged(parts, lane):
    tops = [p[:, :1] for p in parts]
    top = tops[0]
    for t in tops[1:]:
        top = jnp.maximum(top, t)
    total = sum(jnp.exp(t - top) * p for t, p in zip(tops, parts))
    return jnp.where(lane == 0, top, total)


def kernel(
    tok_hbm, gain_hbm, wk_hbm, wv_hbm, query_hbm, gate_hbm, cache, read,
    tok, gain, wk, wv, gate, query, spread, normed, made, gates, packed,
    part, part_in, row, row_in, final, final_in, read_in, lined,
    tok_sem, in_sem, wave_sem, send_sem, recv_sem, up_sem,
):
    me = tuple(lax.axis_index(a) for a in AXES)
    z, x, y, core = me
    apart = 1 - lax.axis_index("gr")
    chip = z * 16 + x * 4 + y
    mine = chip * 2 + core
    sp, tp = z * 4 + x, y * 2 + core

    zs = [across(z, k) for k in range(4)]
    xs = [(x + k) % 4 for k in range(4)]
    ys = [(y + k) % 4 for k in range(4)]
    cores = [core, 1 - core]
    tps = [(yt, ct) for yt in ys for ct in cores]
    sps = [(zt, xt) for zt in zs for xt in xs]

    def tok_copy(i):
        kz, kx = step_of(z, apart, i)
        rows = pl.ds(pl.multiple_of((x + kx) % 4 * ROWS, ROWS), ROWS)
        return pltpu.make_async_copy(tok_hbm.at[across(z, kz), rows], tok.at[i], tok_sem.at[i % 6])

    def in_copy(n, src, dst):
        return pltpu.make_async_copy(src, dst, in_sem.at[n])

    early = [
        in_copy(0, gain_hbm, gain), in_copy(1, wk_hbm, wk), in_copy(2, wv_hbm, wv),
        in_copy(3, gate_hbm, gate),
    ]
    late = in_copy(4, query_hbm, query)
    tok_copy(0).start()
    for copy in early:
        copy.start()
    tok_copy(1).start()

    barrier = pltpu.get_barrier_semaphore()
    last = len(zs) - 1
    is_last = z // last * apart

    @pl.when(is_last == 0)
    def _():
        with jax.named_scope("signals"):
            for zt in zs[::-1]:
                for xt in xs[::-1]:
                    for yt, ct in tps[::-1]:
                        if zt is not zs[0] or xt is not xs[0] or yt is not ys[0] or ct is not core:
                            pl.semaphore_signal(
                                barrier, inc=1, device_id=device_of((zt, xt, yt, ct)), device_id_type=MESH
                            )

    def await_entry():
        pl.semaphore_wait(barrier, 127 - 32 * apart + is_last)

        @pl.when(is_last == 1)
        def _():
            for zt in zs[:0:-1]:
                for xt in xs[::-1]:
                    for yt, ct in tps[::-1]:
                        pl.semaphore_signal(
                            up_sem.at[0], inc=1, device_id=device_of((zt, xt, yt, ct)), device_id_type=MESH
                        )

    def await_last():
        @pl.when((1 - is_last) * apart == 1)
        def _():
            pl.semaphore_wait(up_sem.at[0], 32)

        @pl.when(z * apart == last - 1)
        def _():
            pl.semaphore_signal(
                up_sem.at[1], inc=1, device_id=device_of((last, x, y, core)), device_id_type=MESH
            )

        @pl.when(is_last == 1)
        def _():
            pl.semaphore_wait(up_sem.at[1], 1)

    def send_steps(i, n):
        for j in (4, 5, 2, 3, 6, 7, 0, 1):
            yt, ct = tps[j]
            for s in range(n):
                kz, kx = step_of(z, apart, i + s)
                zt, xt = across(z, kz), (x + kx) % 4

                def one():
                    send(
                        made.at[zt * 32 + xt * 8 + yt * 2 + ct], cache.at[mine],
                        wave_sem.at[(i + s) % BURST], recv_sem.at[0], (zt, xt, yt, ct),
                    )

                if j:
                    one()
                else:
                    pl.when(kz + kx != 0)(one)

    def await_steps(i, n):
        for s in range(n):
            sem = wave_sem.at[(i + s) % BURST]
            kz, kx = step_of(z, apart, i + s)
            await_bytes(made.at[pl.ds(0, 7)], sem)
            pl.when(kz + kx != 0)(lambda sem=sem: await_bytes(made.at[pl.ds(0, 1)], sem))

    def send_gates(to_last):
        for zt in zs:

            def block():
                for xt in xs:
                    for yt in ys:
                        if zt is not zs[0] or xt is not xs[0] or yt is not ys[0]:
                            send(
                                gate.at[zt * 16 + xt * 4 + yt], gates.at[core * 64 + chip],
                                send_sem.at[0], recv_sem.at[1], (zt, xt, yt, core),
                            )

            pl.when(zt // last * apart == int(to_last))(block)

    def project(i, n, ahead=()):
        for s in range(n):
            with jax.named_scope("tokwait"):
                tok_copy(i + s).wait()
        with jax.named_scope("norm"):
            for r in range(0, n * ROWS, 16):
                wide = tok[i + r // ROWS, pl.ds(r % ROWS, 16)].astype(jnp.float32)
                mean = jnp.sum(wide * wide, axis=-1, keepdims=True) * (1.0 / wide.shape[-1])
                scale = lax.rsqrt(mean + NORM_FLOOR)
                normed[pl.ds(r, 16)] = (wide * scale * gain[...]).astype(jnp.bfloat16)

        for copy in ahead:
            copy.wait()
        with jax.named_scope("dots"):
            lhs = normed[pl.ds(0, n * ROWS)]
            keys = jnp.dot(lhs, wk[...], preferred_element_type=jnp.float32)
            values = jnp.dot(lhs, wv[...], preferred_element_type=jnp.float32)
            for s in range(n):
                kz, kx = step_of(z, apart, i + s)
                base = across(z, kz) * 32 + (x + kx) % 4 * 8
                rows = slice(s * ROWS, (s + 1) * ROWS)
                for h in range(4):
                    cols = slice(h * HD, (h + 1) * HD)
                    both = jnp.concatenate([keys[rows, cols], values[rows, cols]], axis=1)
                    both = both.astype(jnp.bfloat16)
                    made[base + 2 * h] = both[:64]
                    made[base + 2 * h + 1] = both[64:]

    mate = (z, x, y, 1 - core)

    pl.when(is_last == 1)(await_entry)
    with jax.named_scope("inputs"):
        early[0].wait()
    project(0, 1, early[1:])
    for i in range(2, 4):
        tok_copy(i).start()
    with jax.named_scope("barrier"):
        pl.when(is_last == 0)(await_entry)
    with jax.named_scope("sendgates"):
        send_gates(False)
    gates[core * 64 + chip] = gate[chip]
    send_steps(0, 1)
    late.start()
    for i in range(4, 6):
        tok_copy(i).start()
    project(1, 1)
    send_steps(1, 1)
    project(2, 2)
    with jax.named_scope("awaitlast"):
        await_last()
    with jax.named_scope("sendgates"):
        send_gates(True)
    send_steps(2, 2)
    for i in range(6, 8):
        tok_copy(i).start()

    @pl.loop(4, STEPS, step=2)
    def _(i):
        @pl.when(i < STEPS - 4)
        def _():
            for n in range(4, 6):
                tok_copy(i + n).start()

        project(i, 2)

        @pl.when(i < BURST)
        def _():
            send_steps(i, 2)

        @pl.when(i == 12)
        def _():
            with jax.named_scope("waitgates"):
                await_bytes(gates.at[pl.ds(0, 63)], recv_sem.at[1])
            held = gates.at[pl.ds(core * 64, 64)]
            send(held, held, send_sem.at[1], recv_sem.at[2], mate)

    late.wait()
    with jax.named_scope("selfpiece"):
        cache[mine] = made[mine]

    lane = lax.broadcasted_iota(jnp.int32, (8, 2 * HD), 1)
    lane16 = lax.broadcasted_iota(jnp.int32, (16, 2 * HD), 1)
    for g in range(4):
        wide = query[g].astype(jnp.float32)
        spread[g] = jnp.zeros(spread.shape[1:], jnp.float32)
        for h in range(4):
            spread[g, h * 8 : (h + 1) * 8, h * 2 * HD : h * 2 * HD + HD] = wide[h * 8 : (h + 1) * 8]

    with jax.named_scope("gatewait"):
        await_bytes(gates.at[pl.ds(0, 64)], recv_sem.at[2])

    with jax.named_scope("attention"):

        @pl.loop(0, 4)
        def _(g):
            for h in range(4):
                for c in range(4):
                    for b in range(2):
                        packed[b, h * 4 + c : h * 4 + c + 1] = gates[b * 64 + g * 16 + c * 4 + h]
            low, high = packed[0], packed[1]
            low_turned, high_turned = (
                jnp.concatenate([t[:, HD:], t[:, :HD]], axis=1) for t in (low, high)
            )
            bias = jnp.where(
                lane16 < HD,
                jnp.where(core == 0, low, low_turned),
                jnp.where(core == 0, high_turned, high),
            )
            pairs = jnp.concatenate(
                [
                    jnp.concatenate(
                        [
                            made[pl.ds(g * 32 + c * 8 + h * 2, 2)].reshape(ROWS, 2 * HD)
                            for h in range(4)
                        ],
                        axis=1,
                    )
                    for c in range(4)
                ],
                axis=0,
            )
            away = jnp.concatenate(
                [
                    jnp.broadcast_to(
                        jnp.concatenate(
                            [bias[h * 4 + c : h * 4 + c + 1] for c in range(4)], axis=1
                        ),
                        (8, 4 * ROWS),
                    )
                    for h in range(4)
                ],
                axis=0,
            )
            score = lax.dot_general(
                spread[g].astype(jnp.bfloat16), pairs, KV, preferred_element_type=jnp.float32
            )
            score = score * HD ** (-0.5) - away
            top = jnp.max(score, axis=1, keepdims=True)
            weight = jnp.exp(score - top)
            total = jnp.sum(weight, axis=1, keepdims=True)
            first = weight.astype(jnp.bfloat16).astype(jnp.float32)
            second = (weight - first).astype(jnp.bfloat16).astype(jnp.float32)
            third = weight - first - second
            split = jnp.concatenate([first, second, third], axis=0).astype(jnp.bfloat16)
            out = jnp.dot(split, pairs, preferred_element_type=jnp.float32)
            out = out[:32] + out[32:64] + out[64:]
            for h in range(4):
                rows = slice(h * 8, (h + 1) * 8)
                part[g * 4 + h] = jnp.where(
                    lane == 0,
                    top[rows],
                    jnp.where(lane < HD, total[rows], out[rows, h * 2 * HD : (h + 1) * 2 * HD]),
                )

    def send_part():
        for yt, ct in tps[1:]:
            send(
                part.at[pl.ds((yt * 2 + ct) * 2, 2)], part_in.at[pl.ds(tp * 2, 2)],
                send_sem.at[2], recv_sem.at[3], (z, x, yt, ct),
            )

    def send_row():
        with jax.named_scope("wait_part"):
            await_bytes(part_in.at[pl.ds(0, 14)], recv_sem.at[3])
        for n in range(2):
            part_in[tp * 2 + n] = part[tp * 2 + n]
        for n in range(2):
            one = merged([part_in[t * 2 + n] for t in range(8)], lane)
            for j in range(8):
                row[n * 8 + j] = one[j : j + 1]

        for zt, xt in sps[1:]:
            send(
                row.at[zt * 4 + xt], row_in.at[sp], send_sem.at[3], recv_sem.at[4],
                (zt, xt, y, core),
            )

    def send_final():
        with jax.named_scope("wait_row"):
            await_bytes(row_in.at[pl.ds(0, 15)], recv_sem.at[4])
        row_in[sp] = row[sp]
        one = merged([row_in[s] for s in range(16)], lane[:1])
        done = one / one[:, 1:2]
        final[0] = done
        final_in[sp] = done

        for zt, xt in sps[1:]:
            send(
                final.at[0], final_in.at[sp], send_sem.at[4], recv_sem.at[5], (zt, xt, y, core)
            )

    def send_read():
        with jax.named_scope("wait_final"):
            await_bytes(final_in.at[pl.ds(0, 15)], recv_sem.at[5])
        for s in range(16):
            read_in[tp, s] = final_in[s]

        for yt, ct in tps[1:]:
            send(final_in, read_in.at[tp], send_sem.at[5], recv_sem.at[6], (z, x, yt, ct))

    at = BURST
    for stage, n in zip((send_part, send_row, send_final, send_read), FOLLOW):
        stage()
        if n:
            with jax.named_scope("pace"):
                await_steps(at - BURST, n)
            send_steps(at, n)
        at += n

    with jax.named_scope("wait_read"):
        await_bytes(read_in.at[pl.ds(0, 7)], recv_sem.at[6])
    for t in range(8):
        for s in range(16):
            lined[s : s + 1] = read_in[t, s]
        read[t // 2, t % 2 * 16 : t % 2 * 16 + 16] = lined[...][:, HD:]

    with jax.named_scope("wait_sent"):
        await_steps(STEPS - BURST, BURST)
    await_bytes(gates.at[pl.ds(0, 63)], send_sem.at[0])
    await_bytes(gates.at[pl.ds(0, 64)], send_sem.at[1])
    await_bytes(part_in.at[pl.ds(0, 14)], send_sem.at[2])
    await_bytes(row_in.at[pl.ds(0, 15)], send_sem.at[3])
    await_bytes(final_in.at[pl.ds(0, 15)], send_sem.at[4])
    await_bytes(read_in.at[pl.ds(0, 7)], send_sem.at[5])
    with jax.named_scope("wait_all"):
        await_bytes(cache.at[pl.ds(0, 127)], recv_sem.at[0])


def store_kernel(cache, read, cache_out, read_out, sem):
    copies = [pltpu.make_async_copy(read, read_out, sem.at[4])] + [
        pltpu.make_async_copy(cache.at[pl.ds(n * 32, 32)], cache_out.at[pl.ds(n * 32, 32)], sem.at[n])
        for n in range(4)
    ]
    for copy in copies:
        copy.start()
    for copy in copies:
        copy.wait()


def shards(tokens, norm_gain, w_key, w_value, new_query, cum_gate):
    width = tokens.shape[-1]
    lanes = 2 * HD
    bf16, f32 = jnp.bfloat16, jnp.float32
    cache, read = pl.pallas_call(
        kernel,
        out_shape=[
            pltpu.VMEM((128, 64, lanes), bf16),
            pltpu.VMEM(new_query.shape, f32),
        ],
        in_specs=[pl.BlockSpec(memory_space=pl.ANY)] * 6,
        out_specs=[pl.BlockSpec(memory_space=pltpu.VMEM)] * 2,
        scratch_shapes=[
            pltpu.VMEM((STEPS, ROWS, width), bf16),
            pltpu.VMEM((1, width), f32),
            pltpu.VMEM(w_key.shape, bf16),
            pltpu.VMEM(w_value.shape, bf16),
            pltpu.VMEM((64, 1, lanes), f32),
            pltpu.VMEM(new_query.shape, bf16),
            pltpu.VMEM((4, 32, 4 * lanes), f32),
            pltpu.VMEM((2 * ROWS, width), bf16),
            pltpu.VMEM((128, 64, lanes), bf16),
            pltpu.VMEM((128, 1, lanes), f32),
            pltpu.VMEM((2, 16, lanes), f32),
            pltpu.VMEM((16, 8, lanes), f32),
            pltpu.VMEM((16, 8, lanes), f32),
            pltpu.VMEM((16, 1, lanes), f32),
            pltpu.VMEM((16, 1, lanes), f32),
            pltpu.VMEM((1, 1, lanes), f32),
            pltpu.VMEM((16, 1, lanes), f32),
            pltpu.VMEM((8, 16, 1, lanes), f32),
            pltpu.VMEM((16, lanes), f32),
            pltpu.SemaphoreType.DMA((6,)),
            pltpu.SemaphoreType.DMA((5,)),
            pltpu.SemaphoreType.DMA((BURST,)),
            pltpu.SemaphoreType.DMA((6,)),
            pltpu.SemaphoreType.DMA((7,)),
            pltpu.SemaphoreType.REGULAR((2,)),
        ],
        compiler_params=pltpu.CompilerParams(collective_id=0, has_side_effects=True),
    )(
        tokens, norm_gain.reshape(1, width), w_key, w_value, new_query,
        cum_gate.reshape(64, 1, lanes),
    )
    cache = pltpu.with_memory_space_constraint(cache, pltpu.VMEM)
    read = pltpu.with_memory_space_constraint(read, pltpu.VMEM)
    kv_cache, first_read = pl.pallas_call(
        store_kernel,
        out_shape=[
            jax.ShapeDtypeStruct(cache.shape, bf16), jax.ShapeDtypeStruct(read.shape, f32)
        ],
        in_specs=[pl.BlockSpec(memory_space=pltpu.VMEM)] * 2,
        out_specs=[pl.BlockSpec(memory_space=pl.ANY)] * 2,
        scratch_shapes=[pltpu.SemaphoreType.DMA((5,))],
    )(cache, read)
    return kv_cache.reshape(1, 1, 128 * 64, lanes), first_read


def solution(mesh):
    split = Mesh(mesh.devices.reshape(mesh.shape["gr"], 4, 4, 4, 2), ("gr", *AXES))
    return jax.shard_map(
        shards,
        mesh=split,
        in_specs=(
            P("gr", (*SP, *TP), None), P(), P(), P(), P("gr", None, None), P(("gr", *SP), TP, None)
        ),
        out_specs=(P(("gr", *SP), TP, None, None), P("gr", None, None)),
        check_vma=False,
    )
```

```python
import jax
import jax.numpy as jnp
from jax import lax
from jax.experimental import pallas as pl
from jax.experimental.pallas import tpu as pltpu
from jax.sharding import Mesh
from jax.sharding import PartitionSpec as P

HD = 64
AXES = ("z", "x", "y", "core")
SP, TP = AXES[:2], AXES[2:]
MESH = pl.DeviceIdType.MESH
NORM_FLOOR = 0.05
ROWS = 128
STEPS = 16
BURST = 6
FOLLOW = (2, 2, 3, 3)
KV = (((1,), (1,)), ((), ()))


def across(z, kz):
    flip = z + 1 - 2 * (z % 2)
    return ((1 - kz % 2) * z + (kz % 2) * flip + 2 * (kz // 2)) % 4


def step_of(z, apart, i):
    j = i % 4
    one, two = z % 2 * (1 - z // 2) * apart + 1 - apart, (1 - z % 2) * (z // 2) * apart
    even = 2 + one + j // 2 * (1 - 2 * one)
    odd = 1 - two + j // 2 * (2 * two - 1)
    return even + j % 2 * (odd - even), (i // 4 + j + 2) % 4


def device_of(t):
    return dict(zip(AXES, t))


def send(src, dst, send_sem, recv_sem, to):
    pltpu.make_async_remote_copy(
        src, dst, send_sem, recv_sem, device_id=device_of(to), device_id_type=MESH
    ).start()


def await_bytes(like, sem):
    pltpu.make_async_copy(like, like, sem).wait()


def merged(parts, lane):
    tops = [p[:, :1] for p in parts]
    top = tops[0]
    for t in tops[1:]:
        top = jnp.maximum(top, t)
    total = sum(jnp.exp(t - top) * p for t, p in zip(tops, parts))
    return jnp.where(lane == 0, top, total)


def kernel(
    tok_hbm, gain_hbm, wk_hbm, wv_hbm, query_hbm, gate_hbm, cache, read,
    tok, gain, wk, wv, gate, query, spread, normed, made, gates, packed,
    part, part_in, row, row_in, final, final_in, read_in, lined,
    tok_sem, in_sem, wave_sem, send_sem, recv_sem, up_sem,
):
    me = tuple(lax.axis_index(a) for a in AXES)
    z, x, y, core = me
    apart = 1 - lax.axis_index("gr")
    chip = z * 16 + x * 4 + y
    mine = chip * 2 + core
    sp, tp = z * 4 + x, y * 2 + core

    zs = [across(z, k) for k in range(4)]
    xs = [(x + k) % 4 for k in range(4)]
    ys = [(y + k) % 4 for k in range(4)]
    cores = [core, 1 - core]
    tps = [(yt, ct) for yt in ys for ct in cores]
    sps = [(zt, xt) for zt in zs for xt in xs]

    def tok_copy(i):
        kz, kx = step_of(z, apart, i)
        rows = pl.ds(pl.multiple_of((x + kx) % 4 * ROWS, ROWS), ROWS)
        return pltpu.make_async_copy(tok_hbm.at[across(z, kz), rows], tok.at[i], tok_sem.at[i % 6])

    def in_copy(n, src, dst):
        return pltpu.make_async_copy(src, dst, in_sem.at[n])

    early = [
        in_copy(0, gain_hbm, gain), in_copy(1, wk_hbm, wk), in_copy(2, wv_hbm, wv),
        in_copy(3, gate_hbm, gate),
    ]
    late = in_copy(4, query_hbm, query)
    tok_copy(0).start()
    for copy in early:
        copy.start()
    tok_copy(1).start()

    barrier = pltpu.get_barrier_semaphore()
    last = len(zs) - 1
    is_last = z // last * apart

    @pl.when(is_last == 0)
    def _():
        with jax.named_scope("signals"):
            for zt in zs[::-1]:
                for xt in xs[::-1]:
                    for yt, ct in tps[::-1]:
                        if zt is not zs[0] or xt is not xs[0] or yt is not ys[0] or ct is not core:
                            pl.semaphore_signal(
                                barrier, inc=1, device_id=device_of((zt, xt, yt, ct)), device_id_type=MESH
                            )

    def await_entry():
        pl.semaphore_wait(barrier, 127 - 32 * apart + is_last)

        @pl.when(is_last == 1)
        def _():
            for zt in zs[:0:-1]:
                for xt in xs[::-1]:
                    for yt, ct in tps[::-1]:
                        pl.semaphore_signal(
                            up_sem.at[0], inc=1, device_id=device_of((zt, xt, yt, ct)), device_id_type=MESH
                        )

    def await_last():
        @pl.when((1 - is_last) * apart == 1)
        def _():
            pl.semaphore_wait(up_sem.at[0], 32)

        @pl.when(z * apart == last - 1)
        def _():
            pl.semaphore_signal(
                up_sem.at[1], inc=1, device_id=device_of((last, x, y, core)), device_id_type=MESH
            )

        @pl.when(is_last == 1)
        def _():
            pl.semaphore_wait(up_sem.at[1], 1)

    def send_steps(i, n):
        for j in (4, 5, 2, 3, 6, 7, 0, 1):
            yt, ct = tps[j]
            for s in range(n):
                kz, kx = step_of(z, apart, i + s)
                zt, xt = across(z, kz), (x + kx) % 4

                def one():
                    send(
                        made.at[zt * 32 + xt * 8 + yt * 2 + ct], cache.at[mine],
                        wave_sem.at[(i + s) % BURST], recv_sem.at[0], (zt, xt, yt, ct),
                    )

                if j:
                    one()
                else:
                    pl.when(kz + kx != 0)(one)

    def await_steps(i, n):
        for s in range(n):
            sem = wave_sem.at[(i + s) % BURST]
            kz, kx = step_of(z, apart, i + s)
            await_bytes(made.at[pl.ds(0, 7)], sem)
            pl.when(kz + kx != 0)(lambda sem=sem: await_bytes(made.at[pl.ds(0, 1)], sem))

    def send_gates(to_last):
        for zt in zs:

            def block():
                for xt in xs:
                    for yt in ys:
                        if zt is not zs[0] or xt is not xs[0] or yt is not ys[0]:
                            send(
                                gate.at[zt * 16 + xt * 4 + yt], gates.at[core * 64 + chip],
                                send_sem.at[0], recv_sem.at[1], (zt, xt, yt, core),
                            )

            pl.when(zt // last * apart == int(to_last))(block)

    def project(i, n, ahead=()):
        for s in range(n):
            with jax.named_scope("tokwait"):
                tok_copy(i + s).wait()
        with jax.named_scope("norm"):
            for r in range(0, n * ROWS, 16):
                wide = tok[i + r // ROWS, pl.ds(r % ROWS, 16)].astype(jnp.float32)
                mean = jnp.sum(wide * wide, axis=-1, keepdims=True) * (1.0 / wide.shape[-1])
                scale = lax.rsqrt(mean + NORM_FLOOR)
                normed[pl.ds(r, 16)] = (wide * scale * gain[...]).astype(jnp.bfloat16)

        for copy in ahead:
            copy.wait()
        with jax.named_scope("dots"):
            lhs = normed[pl.ds(0, n * ROWS)]
            keys = jnp.dot(lhs, wk[...], preferred_element_type=jnp.float32)
            values = jnp.dot(lhs, wv[...], preferred_element_type=jnp.float32)
            for s in range(n):
                kz, kx = step_of(z, apart, i + s)
                base = across(z, kz) * 32 + (x + kx) % 4 * 8
                rows = slice(s * ROWS, (s + 1) * ROWS)
                for h in range(4):
                    cols = slice(h * HD, (h + 1) * HD)
                    both = jnp.concatenate([keys[rows, cols], values[rows, cols]], axis=1)
                    both = both.astype(jnp.bfloat16)
                    made[base + 2 * h] = both[:64]
                    made[base + 2 * h + 1] = both[64:]

    mate = (z, x, y, 1 - core)

    pl.when(is_last == 1)(await_entry)
    with jax.named_scope("inputs"):
        early[0].wait()
    project(0, 1, early[1:])
    for i in range(2, 4):
        tok_copy(i).start()
    with jax.named_scope("barrier"):
        pl.when(is_last == 0)(await_entry)
    with jax.named_scope("sendgates"):
        send_gates(False)
    gates[core * 64 + chip] = gate[chip]
    send_steps(0, 1)
    late.start()
    for i in range(4, 6):
        tok_copy(i).start()
    project(1, 1)
    send_steps(1, 1)
    project(2, 2)
    with jax.named_scope("awaitlast"):
        await_last()
    with jax.named_scope("sendgates"):
        send_gates(True)
    send_steps(2, 2)
    for i in range(6, 8):
        tok_copy(i).start()

    @pl.loop(4, STEPS, step=2)
    def _(i):
        @pl.when(i < STEPS - 4)
        def _():
            for n in range(4, 6):
                tok_copy(i + n).start()

        project(i, 2)

        @pl.when(i < BURST)
        def _():
            send_steps(i, 2)

        @pl.when(i == 12)
        def _():
            with jax.named_scope("waitgates"):
                await_bytes(gates.at[pl.ds(0, 63)], recv_sem.at[1])
            held = gates.at[pl.ds(core * 64, 64)]
            send(held, held, send_sem.at[1], recv_sem.at[2], mate)

    late.wait()
    with jax.named_scope("selfpiece"):
        cache[mine] = made[mine]

    lane = lax.broadcasted_iota(jnp.int32, (8, 2 * HD), 1)
    lane16 = lax.broadcasted_iota(jnp.int32, (16, 2 * HD), 1)
    for g in range(4):
        wide = query[g].astype(jnp.float32)
        spread[g] = jnp.zeros(spread.shape[1:], jnp.float32)
        for h in range(4):
            spread[g, h * 8 : (h + 1) * 8, h * 2 * HD : h * 2 * HD + HD] = wide[h * 8 : (h + 1) * 8]

    with jax.named_scope("gatewait"):
        await_bytes(gates.at[pl.ds(0, 64)], recv_sem.at[2])

    with jax.named_scope("attention"):

        @pl.loop(0, 4)
        def _(g):
            for h in range(4):
                for c in range(4):
                    for b in range(2):
                        packed[b, h * 4 + c : h * 4 + c + 1] = gates[b * 64 + g * 16 + c * 4 + h]
            low, high = packed[0], packed[1]
            low_turned, high_turned = (
                jnp.concatenate([t[:, HD:], t[:, :HD]], axis=1) for t in (low, high)
            )
            bias = jnp.where(
                lane16 < HD,
                jnp.where(core == 0, low, low_turned),
                jnp.where(core == 0, high_turned, high),
            )
            pairs = jnp.concatenate(
                [
                    jnp.concatenate(
                        [
                            made[pl.ds(g * 32 + c * 8 + h * 2, 2)].reshape(ROWS, 2 * HD)
                            for h in range(4)
                        ],
                        axis=1,
                    )
                    for c in range(4)
                ],
                axis=0,
            )
            away = jnp.concatenate(
                [
                    jnp.broadcast_to(
                        jnp.concatenate(
                            [bias[h * 4 + c : h * 4 + c + 1] for c in range(4)], axis=1
                        ),
                        (8, 4 * ROWS),
                    )
                    for h in range(4)
                ],
                axis=0,
            )
            score = lax.dot_general(
                spread[g].astype(jnp.bfloat16), pairs, KV, preferred_element_type=jnp.float32
            )
            score = score * HD ** (-0.5) - away
            top = jnp.max(score, axis=1, keepdims=True)
            weight = jnp.exp(score - top)
            total = jnp.sum(weight, axis=1, keepdims=True)
            first = weight.astype(jnp.bfloat16).astype(jnp.float32)
            second = (weight - first).astype(jnp.bfloat16).astype(jnp.float32)
            third = weight - first - second
            split = jnp.concatenate([first, second, third], axis=0).astype(jnp.bfloat16)
            out = jnp.dot(split, pairs, preferred_element_type=jnp.float32)
            out = out[:32] + out[32:64] + out[64:]
            for h in range(4):
                rows = slice(h * 8, (h + 1) * 8)
                part[g * 4 + h] = jnp.where(
                    lane == 0,
                    top[rows],
                    jnp.where(lane < HD, total[rows], out[rows, h * 2 * HD : (h + 1) * 2 * HD]),
                )

    def send_part():
        for yt, ct in tps[1:]:
            send(
                part.at[pl.ds((yt * 2 + ct) * 2, 2)], part_in.at[pl.ds(tp * 2, 2)],
                send_sem.at[2], recv_sem.at[3], (z, x, yt, ct),
            )

    def send_row():
        with jax.named_scope("wait_part"):
            await_bytes(part_in.at[pl.ds(0, 14)], recv_sem.at[3])
        for n in range(2):
            part_in[tp * 2 + n] = part[tp * 2 + n]
        for n in range(2):
            one = merged([part_in[t * 2 + n] for t in range(8)], lane)
            for j in range(8):
                row[n * 8 + j] = one[j : j + 1]

        for zt, xt in sps[1:]:
            send(
                row.at[zt * 4 + xt], row_in.at[sp], send_sem.at[3], recv_sem.at[4],
                (zt, xt, y, core),
            )

    def send_final():
        with jax.named_scope("wait_row"):
            await_bytes(row_in.at[pl.ds(0, 15)], recv_sem.at[4])
        row_in[sp] = row[sp]
        one = merged([row_in[s] for s in range(16)], lane[:1])
        done = one / one[:, 1:2]
        final[0] = done
        final_in[sp] = done

        for zt, xt in sps[1:]:
            send(
                final.at[0], final_in.at[sp], send_sem.at[4], recv_sem.at[5], (zt, xt, y, core)
            )

    def send_read():
        with jax.named_scope("wait_final"):
            await_bytes(final_in.at[pl.ds(0, 15)], recv_sem.at[5])
        for s in range(16):
            read_in[tp, s] = final_in[s]

        for yt, ct in tps[1:]:
            send(final_in, read_in.at[tp], send_sem.at[5], recv_sem.at[6], (z, x, yt, ct))

    at = BURST
    for stage, n in zip((send_part, send_row, send_final, send_read), FOLLOW):
        stage()
        if n:
            with jax.named_scope("pace"):
                await_steps(at - BURST, n)
            send_steps(at, n)
        at += n

    with jax.named_scope("wait_read"):
        await_bytes(read_in.at[pl.ds(0, 7)], recv_sem.at[6])
    for t in range(8):
        for s in range(16):
            lined[s : s + 1] = read_in[t, s]
        read[t // 2, t % 2 * 16 : t % 2 * 16 + 16] = lined[...][:, HD:]

    with jax.named_scope("wait_sent"):
        await_steps(STEPS - BURST, BURST)
    await_bytes(gates.at[pl.ds(0, 63)], send_sem.at[0])
    await_bytes(gates.at[pl.ds(0, 64)], send_sem.at[1])
    await_bytes(part_in.at[pl.ds(0, 14)], send_sem.at[2])
    await_bytes(row_in.at[pl.ds(0, 15)], send_sem.at[3])
    await_bytes(final_in.at[pl.ds(0, 15)], send_sem.at[4])
    await_bytes(read_in.at[pl.ds(0, 7)], send_sem.at[5])
    with jax.named_scope("wait_all"):
        await_bytes(cache.at[pl.ds(0, 127)], recv_sem.at[0])


def store_kernel(cache, read, cache_out, read_out, sem):
    copies = [pltpu.make_async_copy(read, read_out, sem.at[4])] + [
        pltpu.make_async_copy(cache.at[pl.ds(n * 32, 32)], cache_out.at[pl.ds(n * 32, 32)], sem.at[n])
        for n in range(4)
    ]
    for copy in copies:
        copy.start()
    for copy in copies:
        copy.wait()


def shards(tokens, norm_gain, w_key, w_value, new_query, cum_gate):
    width = tokens.shape[-1]
    lanes = 2 * HD
    bf16, f32 = jnp.bfloat16, jnp.float32
    cache, read = pl.pallas_call(
        kernel,
        out_shape=[
            pltpu.VMEM((128, 64, lanes), bf16),
            pltpu.VMEM(new_query.shape, f32),
        ],
        in_specs=[pl.BlockSpec(memory_space=pl.ANY)] * 6,
        out_specs=[pl.BlockSpec(memory_space=pltpu.VMEM)] * 2,
        scratch_shapes=[
            pltpu.VMEM((STEPS, ROWS, width), bf16),
            pltpu.VMEM((1, width), f32),
            pltpu.VMEM(w_key.shape, bf16),
            pltpu.VMEM(w_value.shape, bf16),
            pltpu.VMEM((64, 1, lanes), f32),
            pltpu.VMEM(new_query.shape, bf16),
            pltpu.VMEM((4, 32, 4 * lanes), f32),
            pltpu.VMEM((2 * ROWS, width), bf16),
            pltpu.VMEM((128, 64, lanes), bf16),
            pltpu.VMEM((128, 1, lanes), f32),
            pltpu.VMEM((2, 16, lanes), f32),
            pltpu.VMEM((16, 8, lanes), f32),
            pltpu.VMEM((16, 8, lanes), f32),
            pltpu.VMEM((16, 1, lanes), f32),
            pltpu.VMEM((16, 1, lanes), f32),
            pltpu.VMEM((1, 1, lanes), f32),
            pltpu.VMEM((16, 1, lanes), f32),
            pltpu.VMEM((8, 16, 1, lanes), f32),
            pltpu.VMEM((16, lanes), f32),
            pltpu.SemaphoreType.DMA((6,)),
            pltpu.SemaphoreType.DMA((5,)),
            pltpu.SemaphoreType.DMA((BURST,)),
            pltpu.SemaphoreType.DMA((6,)),
            pltpu.SemaphoreType.DMA((7,)),
            pltpu.SemaphoreType.REGULAR((2,)),
        ],
        compiler_params=pltpu.CompilerParams(collective_id=0, has_side_effects=True),
    )(
        tokens, norm_gain.reshape(1, width), w_key, w_value, new_query,
        cum_gate.reshape(64, 1, lanes),
    )
    cache = pltpu.with_memory_space_constraint(cache, pltpu.VMEM)
    read = pltpu.with_memory_space_constraint(read, pltpu.VMEM)
    kv_cache, first_read = pl.pallas_call(
        store_kernel,
        out_shape=[
            jax.ShapeDtypeStruct(cache.shape, bf16), jax.ShapeDtypeStruct(read.shape, f32)
        ],
        in_specs=[pl.BlockSpec(memory_space=pltpu.VMEM)] * 2,
        out_specs=[pl.BlockSpec(memory_space=pl.ANY)] * 2,
        scratch_shapes=[pltpu.SemaphoreType.DMA((5,))],
    )(cache, read)
    return kv_cache.reshape(1, 1, 128 * 64, lanes), first_read


def solution(mesh):
    split = Mesh(mesh.devices.reshape(mesh.shape["gr"], 4, 4, 4, 2), ("gr", *AXES))
    return jax.shard_map(
        shards,
        mesh=split,
        in_specs=(
            P("gr", (*SP, *TP), None), P(), P(), P(), P("gr", None, None), P(("gr", *SP), TP, None)
        ),
        out_specs=(P(("gr", *SP), TP, None, None), P("gr", None, None)),
        check_vma=False,
    )
```
